32 devices in a mesh: rep: 2 (over x), fs: 8 (over z, y), tp: 2 (over core).
Axes of the slice: x: 2, y: 2, z: 4, core: 2. Of those that a mesh axis runs over, the one named last changes fastest.
Arguments:
- incoming_features: bfloat16 [3072, 2048], P(('rep', 'fs'), 'tp'), may hold values from -6 to 6
- attend_prenormal_scale: bfloat16 [2048], replicated, may hold values from 0.099609375 to 1.8984375
- probe_matrix: bfloat16 [2048, 512], P('fs', 'tp'), may hold values from -0.125 to 0.125
- lookup_matrix: bfloat16 [2048, 512], P('fs', 'tp'), may hold values from -0.125 to 0.125
- content_matrix: bfloat16 [2048, 1024], P('fs', 'tp'), may hold values from -0.125 to 0.125
- forgetting_matrix: bfloat16 [2048, 512], P('fs', 'tp'), may hold values from -0.125 to 0.125
- result_switch_matrix: bfloat16 [2048, 1024], P('fs', 'tp'), may hold values from -0.125 to 0.125
- forgetting_shift: float32 [512], P('tp'), may hold values from -0.5 to 5.5
- spike_forget_logarithm: float32 [3072, 512], P(('rep', 'fs'), 'tp'), may hold values from -0.7 to 0
- attend_unit_scale: bfloat16 [1024], P('tp'), may hold values from 0.099609375 to 1.8984375
- attend_result_matrix: bfloat16 [1024, 2048], P('tp', 'fs'), may hold values from -0.1875 to 0.1875
- perceptron_scale: bfloat16 [2048], replicated, may hold values from 0.099609375 to 1.8984375
- content_expand_matrix: bfloat16 [2048, 4096], P('fs', 'tp'), may hold values from -0.125 to 0.125
- switch_expand_matrix: bfloat16 [2048, 4096], P('fs', 'tp'), may hold values from -0.125 to 0.125
- content_kernel: bfloat16 [3, 4096], P(None, 'tp'), may hold values from -3.5 to 3.5
- switch_kernel: bfloat16 [3, 4096], P(None, 'tp'), may hold values from -3.5 to 3.5
- contract_matrix: bfloat16 [4096, 2048], P('tp', 'fs'), may hold values from -0.09375 to 0.09375
Outputs:
- out_rows: bfloat16 [3072, 2048], P(('rep', 'fs'), 'tp')
The draws below stay inside these ranges and needn't reach their ends.
All inputs are finite; a program needn't handle non-finite values.
Results may differ from the reference program's by a relative error of at most 0.02.
Values may be sent and summed in bfloat16 or wider, within the bound.
A program may use at most 64 MiB of HBM per device.

```python
import math
import jax
import jax.numpy as jnp
from jax import lax

EMBED_DIM = 2048
HEAD_K = 32
HEAD_V = 64
FF = 4096
BLOCK = 64
CONTEXT_SPAN = 192
LOOKUP_FEATURES = 512
VAL_W = 1024
BATCH_SIZE = 16
TOKENS = 3072
N_TP = 2


def draw_forgetting_shift(key, part):
    head_count = LOOKUP_FEATURES // HEAD_K
    key_slow, key_high, key_low = jax.random.split(jax.random.fold_in(key, 11), 3)
    slow = jax.random.uniform(key_slow, (head_count,)) < 0.5
    slow_channels = jnp.repeat(slow, HEAD_K)
    high = jax.random.uniform(key_high, (LOOKUP_FEATURES,), jnp.float32, 3.5, 5.5)
    low = jax.random.uniform(key_low, (LOOKUP_FEATURES,), jnp.float32, -0.5, 1.0)
    return jnp.where(slow_channels, high, low).astype(jnp.float32)


def draw_spike_forget_logarithm(key, part):
    head_count = LOOKUP_FEATURES // HEAD_K
    key_hit, key_depth = jax.random.split(jax.random.fold_in(key, 23))
    hits = jax.random.uniform(key_hit, (TOKENS, head_count)) < 6.0 / CONTEXT_SPAN
    depth = jax.random.uniform(key_depth, (TOKENS, head_count), jnp.float32, math.log(0.5), math.log(0.8))
    return jnp.repeat(jnp.where(hits, depth, 0.0), HEAD_K, axis=1).astype(jnp.float32)


def level_of(own_key, shape, pieces, smallest, top_value):
    factor_of, own = 1.0, jax.random.fold_in(own_key, 6)
    for position, parts in pieces:
        steps = jnp.exp(jax.random.uniform(jax.random.fold_in(own, position), (parts,), jnp.float32, smallest / len(pieces), top_value / len(pieces)))
        factor_of = factor_of * jnp.repeat(steps, shape[position] // parts).reshape([-1 if axis == position else 1 for axis in range(len(shape))])
    return factor_of


def gaussian(own_key, dims, spread, limit, cuts=(), held_as=jnp.bfloat16):
    factor_of = level_of(own_key, dims, cuts, -0.22, 0.18) if cuts else 1.0
    values = jax.random.normal(own_key, dims, jnp.float32) * spread * factor_of
    return jnp.minimum(jnp.maximum(values, -limit), limit).astype(held_as)


def setup_inputs(seed: int = 0) -> dict:
    streams_of = jax.random.split(jax.random.key(seed), 18)
    incoming_features = gaussian(streams_of[0], (TOKENS, EMBED_DIM), 1.0, 6.0, ((0, 16), (1, 2)))
    attend_prenormal_scale = jnp.clip(1.0 + 0.18 * jax.random.normal(streams_of[1], (EMBED_DIM,), jnp.float32), 0.099609375, 1.8984375).astype(jnp.bfloat16)
    probe_matrix = gaussian(streams_of[2], (EMBED_DIM, LOOKUP_FEATURES), EMBED_DIM ** -0.5, 0.125, ((0, 8), (1, 2)))
    lookup_matrix = gaussian(streams_of[3], (EMBED_DIM, LOOKUP_FEATURES), EMBED_DIM ** -0.5, 0.125, ((0, 8), (1, 2)))
    content_matrix = gaussian(streams_of[4], (EMBED_DIM, VAL_W), EMBED_DIM ** -0.5, 0.125, ((0, 8), (1, 2)))
    forgetting_matrix = gaussian(streams_of[5], (EMBED_DIM, LOOKUP_FEATURES), EMBED_DIM ** -0.5, 0.125, ((0, 8), (1, 2)))
    result_switch_matrix = gaussian(streams_of[6], (EMBED_DIM, VAL_W), EMBED_DIM ** -0.5, 0.125, ((0, 8), (1, 2)))
    forgetting_shift = draw_forgetting_shift(jax.random.fold_in(streams_of[17], 71), 0)
    spike_forget_logarithm = draw_spike_forget_logarithm(jax.random.fold_in(streams_of[17], 71), 0)
    attend_unit_scale = jnp.clip(1.0 + 0.18 * jax.random.normal(streams_of[9], (VAL_W,), jnp.float32), 0.099609375, 1.8984375).astype(jnp.bfloat16)
    attend_result_matrix = gaussian(streams_of[10], (VAL_W, EMBED_DIM), VAL_W ** -0.5, 0.1875, ((0, 2), (1, 8)))
    perceptron_scale = jnp.clip(1.0 + 0.18 * jax.random.normal(streams_of[11], (EMBED_DIM,), jnp.float32), 0.099609375, 1.8984375).astype(jnp.bfloat16)
    content_expand_matrix = gaussian(streams_of[12], (EMBED_DIM, FF), EMBED_DIM ** -0.5, 0.125, ((0, 8), (1, 2)))
    switch_expand_matrix = gaussian(streams_of[13], (EMBED_DIM, FF), EMBED_DIM ** -0.5, 0.125, ((0, 8), (1, 2)))
    content_kernel = gaussian(streams_of[14], (3, FF), 3 ** -0.5, 3.5, ((1, 2),))
    switch_kernel = gaussian(streams_of[15], (3, FF), 3 ** -0.5, 3.5, ((1, 2),))
    contract_matrix = gaussian(streams_of[16], (FF, EMBED_DIM), FF ** -0.5, 0.09375, ((0, 2), (1, 8)))
    return {"incoming_features": incoming_features, "attend_prenormal_scale": attend_prenormal_scale, "probe_matrix": probe_matrix, "lookup_matrix": lookup_matrix, "content_matrix": content_matrix, "forgetting_matrix": forgetting_matrix, "result_switch_matrix": result_switch_matrix, "forgetting_shift": forgetting_shift, "spike_forget_logarithm": spike_forget_logarithm, "attend_unit_scale": attend_unit_scale, "attend_result_matrix": attend_result_matrix, "perceptron_scale": perceptron_scale, "content_expand_matrix": content_expand_matrix, "switch_expand_matrix": switch_expand_matrix, "content_kernel": content_kernel, "switch_kernel": switch_kernel, "contract_matrix": contract_matrix}


norm_eps = 1e-06
switch_multiplier = 16.0

def row_norm(content_tokens, gain):
    content_tokens = content_tokens.astype(jnp.float32)
    scaled = content_tokens * lax.rsqrt(lax.optimization_barrier(jnp.mean(content_tokens * content_tokens, axis=-1, keepdims=True)) + norm_eps)
    return (scaled * gain.astype(jnp.float32)).astype(jnp.bfloat16)

def gated_scan(probe_tokens, lookup_tokens, content_tokens, forgetting_scores):
    length, heads, key_size = probe_tokens.shape
    value_size = content_tokens.shape[-1]
    blocks = length // BLOCK

    def split_blocks(array):
        return array.reshape(blocks, BLOCK, heads, array.shape[-1])
    causal = jnp.arange(BLOCK)[:, None] >= jnp.arange(BLOCK)[None, :]
    highest = lax.Precision.HIGHEST

    def step(state, incoming_tokens):
        query_block, key_block, value_block, decay_block = incoming_tokens
        cumulative = jnp.cumsum(decay_block, axis=0)
        differ = cumulative[:, None] - cumulative[None, :]
        weight = jnp.exp(jnp.where(causal[:, :, None, None], differ, -jnp.inf))
        scores = jnp.einsum('thd,shd,tshd->tsh', query_block, key_block, weight, precision=highest)
        inner = jnp.einsum('tsh,shv->thv', scores, value_block, precision=highest)
        carried = jnp.einsum('thd,hdv->thv', query_block * jnp.exp(cumulative), state, precision=highest)
        final = cumulative[-1]
        state = jnp.exp(final)[:, :, None] * state + jnp.einsum('shd,shv->hdv', key_block * jnp.exp(final[None] - cumulative), value_block, precision=highest)
        return (state, inner + carried)
    start_state = jnp.zeros((heads, key_size, value_size), jnp.float32)
    _, result_tokens = lax.scan(step, start_state, (split_blocks(probe_tokens), split_blocks(lookup_tokens), split_blocks(content_tokens), split_blocks(forgetting_scores)))
    return result_tokens.reshape(length, heads, value_size)

def attend_unit_results(probe_tokens, lookup_tokens, content_tokens, result_switch, forgetting_raw, spike_forgetting, attend_unit_scale):
    length = probe_tokens.shape[0]
    heads = probe_tokens.shape[1] // HEAD_K
    forgetting_scores = jax.nn.log_sigmoid(forgetting_raw) / switch_multiplier + spike_forgetting

    def split_heads(array, width):
        return array.astype(jnp.float32).reshape(length, heads, width)
    result_tokens = gated_scan(split_heads(probe_tokens, HEAD_K) * HEAD_K ** (-0.5), split_heads(lookup_tokens, HEAD_K), split_heads(content_tokens, HEAD_V), split_heads(forgetting_scores, HEAD_K))
    result_tokens = result_tokens * lax.rsqrt(lax.optimization_barrier(jnp.mean(result_tokens * result_tokens, axis=-1, keepdims=True)) + norm_eps)
    result_tokens = result_tokens * attend_unit_scale.astype(jnp.float32).reshape(heads, HEAD_V)
    switched_result = result_tokens.reshape(length, heads * HEAD_V) * jax.nn.silu(result_switch.astype(jnp.float32))
    return switched_result.astype(jnp.bfloat16)

def causal_conv(content_tokens, taps):
    content_tokens = content_tokens.astype(jnp.float32)
    taps = taps.astype(jnp.float32)
    width = taps.shape[0]
    padded = jnp.pad(content_tokens, ((width - 1, 0), (0, 0)))
    total = jnp.zeros_like(content_tokens)
    for offset in range(width):
        total = total + padded[offset:offset + content_tokens.shape[0]] * taps[offset]
    return total

def grouped_product(content_tokens, weight):
    group = content_tokens.shape[1] // N_TP
    total = jnp.zeros((content_tokens.shape[0], weight.shape[1]), jnp.float32)
    for index in range(N_TP):
        partial_sum = jnp.dot(content_tokens[:, index * group:(index + 1) * group], weight[index * group:(index + 1) * group], preferred_element_type=jnp.float32)
        total = total + lax.optimization_barrier(partial_sum.astype(jnp.bfloat16)).astype(jnp.float32)
    return total.astype(jnp.bfloat16)

def reference(incoming_features, attend_prenormal_scale, probe_matrix, lookup_matrix, content_matrix, forgetting_matrix, result_switch_matrix, forgetting_shift, spike_forget_logarithm, attend_unit_scale, attend_result_matrix, perceptron_scale, content_expand_matrix, switch_expand_matrix, content_kernel, switch_kernel, contract_matrix):

    def lone_context(incoming_tokens):
        weight_fragments, spike_forgetting = incoming_tokens
        normed = row_norm(weight_fragments, attend_prenormal_scale)
        probe_tokens = jnp.dot(normed, probe_matrix, preferred_element_type=jnp.float32).astype(jnp.bfloat16)
        lookup_tokens = jnp.dot(normed, lookup_matrix, preferred_element_type=jnp.float32).astype(jnp.bfloat16)
        content_tokens = jnp.dot(normed, content_matrix, preferred_element_type=jnp.float32).astype(jnp.bfloat16)
        result_switch = jnp.dot(normed, result_switch_matrix, preferred_element_type=jnp.float32).astype(jnp.bfloat16)
        forgetting_raw = jnp.dot(normed, forgetting_matrix, preferred_element_type=jnp.float32) + forgetting_shift
        switched_result = attend_unit_results(probe_tokens, lookup_tokens, content_tokens, result_switch, forgetting_raw, spike_forgetting, attend_unit_scale)
        mix = grouped_product(switched_result, attend_result_matrix)
        middle = (weight_fragments.astype(jnp.float32) + lax.optimization_barrier(mix).astype(jnp.float32)).astype(jnp.bfloat16)
        normed_mid = row_norm(middle, perceptron_scale)
        up_value = jnp.dot(normed_mid, content_expand_matrix, preferred_element_type=jnp.float32).astype(jnp.bfloat16)
        up_gate = jnp.dot(normed_mid, switch_expand_matrix, preferred_element_type=jnp.float32).astype(jnp.bfloat16)
        conv_value = causal_conv(up_value, content_kernel)
        conv_gated = causal_conv(up_gate, switch_kernel)
        hidden = (conv_value * jax.nn.gelu(conv_gated, approximate=True)).astype(jnp.bfloat16)
        ffn = grouped_product(hidden, contract_matrix)
        return (middle.astype(jnp.float32) + lax.optimization_barrier(ffn).astype(jnp.float32)).astype(jnp.bfloat16)
    result_tokens = lax.map(lone_context, (incoming_features.reshape(BATCH_SIZE, CONTEXT_SPAN, EMBED_DIM), spike_forget_logarithm.reshape(BATCH_SIZE, CONTEXT_SPAN, LOOKUP_FEATURES)))
    return result_tokens.reshape(TOKENS, EMBED_DIM)
```

```python
import functools

import jax
import jax.numpy as jnp
from jax import lax
from jax.experimental import pallas as pl
from jax.experimental.pallas import tpu as pltpu
from jax.sharding import PartitionSpec as P

HEAD_K = 32
HEAD_V = 64
SUB = 16

norm_eps = 1e-06
switch_multiplier = 16.0
MESH = pl.DeviceIdType.MESH
F32 = jnp.float32
BF16 = jnp.bfloat16
VMEM_LIMIT = 60 * 1024 * 1024


def row_norm(content_tokens, gain):
    content_tokens = content_tokens.astype(F32)
    scaled = content_tokens * lax.rsqrt(
        jnp.mean(content_tokens * content_tokens, axis=-1, keepdims=True) + norm_eps
    )
    return (scaled * gain.astype(F32)).astype(BF16)


def factor(n):
    inner = 1
    for size in range(1, n + 1):
        if n % size == 0 and size * size <= n:
            inner = size
    return n // inner, inner


def place(ref, axis, index, size):
    at = pl.ds(pl.multiple_of(index * size, size), size)
    return ref.at[at, :] if axis == 0 else ref.at[:, at]


def send_to(source, target, send_sem, recv_sem, peer):
    copy = pltpu.make_async_remote_copy(
        src_ref=source,
        dst_ref=target,
        send_sem=send_sem,
        recv_sem=recv_sem,
        device_id=peer,
        device_id_type=MESH,
    )
    copy.start()
    return copy


def pieces_of(rows, most):
    for count in range(most, 1, -1):
        if rows % (16 * count) == 0:
            return count
    return 1


def first_half(
    project, result, expand, contract, features, gain, shift, spike, scale, axis, inside, sizes
):
    n_rep, n_fs, n_tp = sizes
    outer, inner = factor(n_fs)
    length, columns = features.shape
    rows = length * n_rep
    heads = shift.shape[0] // HEAD_K
    value_lanes = heads * HEAD_V
    group = n_rep * n_tp
    most = max(n_rep, n_tp)
    weights = (project, result, expand, contract)
    axes = (0, axis, 0, axis)
    splits = (2, 1, 4, 4)
    full = []
    chunks = []
    for w in range(4):
        shape = list(weights[w].shape)
        size = shape[0]
        shape[axes[w]] *= n_fs
        full.append(tuple(shape))
        split = pieces_of(size, splits[w])
        chunks += [(w, k * (size // split), size // split) for k in range(split)]
    count = len(chunks)

    def kernel(*refs):
        sources = refs[:4]
        features_ref, gain_ref, shift_ref, spike_ref, scale_ref = refs[4:9]
        if inside:
            expand_out, contract_out, middle_ref, mid_ref = refs[9:13]
            rest = refs[13:]
            result_out, gated_ref, partial_ref, slot_a, held, slot_b = rest[:6]
            rest = rest[6:]
        else:
            expand_out, contract_out, result_out, gated_ref = refs[9:13]
            rest = refs[13:]
        project_out, whole_ref = rest[:2]
        far_send, far_recv, near_send, near_recv, own_sem, group_send, group_recv = rest[2:9]
        if inside:
            sum_send, sum_recv = rest[9:]
        outs = (project_out, result_out, expand_out, contract_out)
        rep, fs, tp = lax.axis_index("rep"), lax.axis_index("fs"), lax.axis_index("tp")
        a, b = fs // inner, lax.rem(fs, inner)
        far = [lax.rem(a + d, outer) * inner + b for d in range(1, outer)]
        near = [a * inner + lax.rem(b + d, inner) for d in range(1, inner)]
        peers = [{"fs": index} for index in far + near]
        others = [
            {"rep": lax.rem(rep + i, n_rep), "tp": lax.rem(tp + j, n_tp)}
            for i in range(n_rep)
            for j in range(n_tp)
            if i or j
        ]
        barrier = pltpu.get_barrier_semaphore()
        for peer in peers + others:
            pl.semaphore_signal(barrier, inc=1, device_id=peer, device_id_type=MESH)
        pl.semaphore_wait(barrier, len(peers) + len(others))

        def block(w, start, size, index):
            across = weights[w].shape[axes[w]]
            offset = pl.multiple_of(index * across, across)
            if axes[w] == 0:
                return outs[w].at[pl.ds(offset + start, size), :]
            return outs[w].at[pl.ds(start, size), pl.ds(offset, across)]

        far_copies, near_copies, own_copies = {}, {}, {}

        def launch_far(c):
            w, start, size = chunks[c]
            source, target = sources[w].at[pl.ds(start, size), :], block(w, start, size, fs)
            far_copies[c] = [
                send_to(source, target, far_send.at[c, d], far_recv.at[c, d], {"fs": index})
                for d, index in enumerate(far)
            ]

        def launch_near(c):
            w, start, size = chunks[c]
            source, target = sources[w].at[pl.ds(start, size), :], block(w, start, size, fs)
            near_copies[c] = [
                send_to(
                    source, target, near_send.at[c, 0, e], near_recv.at[c, 0, e], {"fs": index}
                )
                for e, index in enumerate(near)
            ]
            own_copies[c] = pltpu.make_async_copy(source, target, own_sem.at[c])
            own_copies[c].start()

        def forward(c):
            w, start, size = chunks[c]
            for d in range(1, outer):
                far_copies[c][d - 1].wait_recv()
                held_block = block(w, start, size, lax.rem(a + outer - d, outer) * inner + b)
                near_copies[c] += [
                    send_to(
                        held_block,
                        held_block,
                        near_send.at[c, d, e],
                        near_recv.at[c, d, e],
                        {"fs": index},
                    )
                    for e, index in enumerate(near)
                ]

        def arrived(c):
            for copy in near_copies[c]:
                copy.wait_recv()
            own_copies[c].wait()

        first = [c for c in range(count) if chunks[c][0] == 0]
        second = [c for c in range(count) if chunks[c][0] == 1]
        later = [c for c in range(count) if chunks[c][0] > 1]

        spot = whole_ref.at[
            pl.ds(pl.multiple_of(rep * length, length), length),
            pl.ds(pl.multiple_of(tp * columns, columns), columns),
        ]
        own = pltpu.make_async_copy(features_ref, spot, own_sem.at[count])
        own.start()
        group_copies = [
            send_to(features_ref, spot, group_send.at[d], group_recv.at[d], peer)
            for d, peer in enumerate(others)
        ]
        for c in first:
            launch_far(c)
            launch_near(c)
        for c in second + later:
            launch_far(c)
        for c in first:
            forward(c)
        for c in second + later:
            launch_near(c)
        for c in first:
            arrived(c)
        own.wait()
        for copy in group_copies:
            copy.wait()

        def sequence(i, carry):
            at = pl.ds(pl.multiple_of(i * length, length), length)
            normed = row_norm(whole_ref[at, :], gain_ref[...])
            sums = jnp.dot(normed, project_out[...], preferred_element_type=F32)
            gated_ref[at, :] = attend_rows(
                sums, shift_ref[...], spike_ref[at, :], scale_ref[...], heads
            )
            return carry

        lax.fori_loop(0, n_rep, sequence, 0)
        for c in second:
            forward(c)
        waiting = list(later)
        for c in waiting[:1]:
            forward(c)
        waiting = waiting[1:]
        for c in second:
            arrived(c)
        if inside:

            def mixer(i, carry):
                at = pl.ds(pl.multiple_of(i * length, length), length)
                partial_ref[at, :] = jnp.dot(
                    gated_ref[at, :], result_out[...], preferred_element_type=F32
                ).astype(BF16)
                return carry

            lax.fori_loop(0, n_rep, mixer, 0)

            def between(stage):
                if stage in (1, 2):
                    forward(waiting.pop(0))

            reduce_steps(
                partial_ref,
                features_ref,
                middle_ref,
                mid_ref,
                slot_a,
                held,
                slot_b,
                sum_send,
                sum_recv,
                sizes,
                between,
            )
        for c in waiting:
            forward(c)
        for c in later:
            arrived(c)
        for c in range(count):
            for copy in far_copies[c] + near_copies[c]:
                copy.wait_send()

    dma = pltpu.SemaphoreType.DMA
    vmem = pl.BlockSpec(memory_space=pltpu.VMEM)
    hbm = pl.BlockSpec(memory_space=pl.ANY)
    out_shape = [jax.ShapeDtypeStruct(full[2], BF16), jax.ShapeDtypeStruct(full[3], BF16)]
    scratch = []
    gated_shape = (rows, value_lanes)
    if inside:
        out_shape += [
            jax.ShapeDtypeStruct((length, columns), BF16),
            jax.ShapeDtypeStruct((rows, columns * n_tp), BF16),
        ]
        out_specs = [hbm, hbm, vmem, vmem]
        scratch += [
            pltpu.VMEM(full[1], BF16),
            pltpu.VMEM(gated_shape, BF16),
            pltpu.VMEM((rows, columns * n_tp), BF16),
            pltpu.VMEM((max(n_tp - 1, 1), rows, columns), BF16),
            pltpu.VMEM((rows, columns), BF16),
            pltpu.VMEM((max(n_rep - 1, 1), length, columns), BF16),
        ]
    else:
        out_shape += [
            jax.ShapeDtypeStruct(full[1], BF16),
            jax.ShapeDtypeStruct(gated_shape, BF16),
        ]
        out_specs = [hbm, hbm, hbm, vmem]
    scratch += [
        pltpu.VMEM(full[0], BF16),
        pltpu.VMEM((rows, columns * n_tp), BF16),
        dma((count, max(outer - 1, 1))),
        dma((count, max(outer - 1, 1))),
        dma((count, outer, max(inner - 1, 1))),
        dma((count, outer, max(inner - 1, 1))),
        dma((count + 1,)),
        dma((group,)),
        dma((group,)),
    ]
    if inside:
        scratch += [dma((4, most)), dma((4, most))]
    return pl.pallas_call(
        kernel,
        out_shape=out_shape,
        in_specs=[vmem] * 9,
        out_specs=out_specs,
        scratch_shapes=scratch,
        compiler_params=pltpu.CompilerParams(
            collective_id=0, has_side_effects=True, vmem_limit_bytes=VMEM_LIMIT
        ),
        name="first_half",
    )(
        *weights,
        features,
        gain.reshape(1, -1),
        shift.reshape(1, -1),
        spike,
        scale.astype(F32).reshape(1, -1),
    )


def reduce_steps(
    part_ref, base_ref, out_ref, all_ref, slot_a, held, slot_b, send_sem, recv_sem, sizes, between
):
    n_rep, n_fs, n_tp = sizes
    rows, columns = base_ref.shape
    rep, tp = lax.axis_index("rep"), lax.axis_index("tp")
    tps = [lax.rem(tp + d, n_tp) for d in range(1, n_tp)]
    reps = [lax.rem(rep + d, n_rep) for d in range(1, n_rep)]

    def send(stage, d, source, target, peer):
        return send_to(source, target, send_sem.at[stage, d], recv_sem.at[stage, d], peer)

    copies = [
        send(0, d, place(part_ref, 1, index, columns), slot_a.at[d], {"tp": index})
        for d, index in enumerate(tps)
    ]
    for copy in copies:
        copy.wait()
    total = place(part_ref, 1, tp, columns)[...].astype(F32)
    for d in range(len(tps)):
        total = total + slot_a[d].astype(F32)
    held[...] = total.astype(BF16)
    copies = [
        send(1, d, place(held, 0, index, rows), slot_b.at[d], {"rep": index})
        for d, index in enumerate(reps)
    ]
    between(1)
    for copy in copies:
        copy.wait()
    total = place(held, 0, rep, rows)[...].astype(F32)
    for d in range(len(reps)):
        total = total + slot_b[d].astype(F32)
    result = (base_ref[...].astype(F32) + total.astype(BF16).astype(F32)).astype(BF16)
    out_ref[...] = result
    if all_ref is not None:
        block = all_ref.at[
            pl.ds(pl.multiple_of(rep * rows, rows), rows),
            pl.ds(pl.multiple_of(tp * columns, columns), columns),
        ]
        block[...] = result
        copies = [send(2, d, block, block, {"rep": index}) for d, index in enumerate(reps)]
        between(2)
        for copy in copies:
            copy.wait()
        strip = place(all_ref, 1, tp, columns)
        copies = [send(3, d, strip, strip, {"tp": index}) for d, index in enumerate(tps)]
        for copy in copies:
            copy.wait()


def reduce_group(partial, base, sizes, spread, collective_id):
    n_rep, n_fs, n_tp = sizes
    rows, columns = base.shape

    def kernel(*refs):
        part_ref, base_ref = refs[:2]
        if spread:
            out_ref, all_ref, slot_a, held, slot_b, send_sem, recv_sem = refs[2:]
        else:
            all_ref = None
            out_ref, slot_a, held, slot_b, send_sem, recv_sem = refs[2:]
        rep, tp = lax.axis_index("rep"), lax.axis_index("tp")
        barrier = pltpu.get_barrier_semaphore()
        for d in range(1, n_tp):
            peer = {"tp": lax.rem(tp + d, n_tp)}
            pl.semaphore_signal(barrier, inc=1, device_id=peer, device_id_type=MESH)
        for d in range(1, n_rep):
            peer = {"rep": lax.rem(rep + d, n_rep)}
            pl.semaphore_signal(barrier, inc=1, device_id=peer, device_id_type=MESH)
        pl.semaphore_wait(barrier, n_tp + n_rep - 2)
        reduce_steps(
            part_ref,
            base_ref,
            out_ref,
            all_ref,
            slot_a,
            held,
            slot_b,
            send_sem,
            recv_sem,
            sizes,
            lambda stage: None,
        )

    out_shape = [jax.ShapeDtypeStruct((rows, columns), BF16)]
    if spread:
        out_shape.append(jax.ShapeDtypeStruct((rows * n_rep, columns * n_tp), BF16))
    vmem = pl.BlockSpec(memory_space=pltpu.VMEM)
    most = max(n_rep, n_tp)
    return pl.pallas_call(
        kernel,
        out_shape=out_shape,
        in_specs=[vmem, vmem],
        out_specs=[vmem] * len(out_shape),
        scratch_shapes=[
            pltpu.VMEM((max(n_tp - 1, 1), rows * n_rep, columns), BF16),
            pltpu.VMEM((rows * n_rep, columns), BF16),
            pltpu.VMEM((max(n_rep - 1, 1), rows, columns), BF16),
            pltpu.SemaphoreType.DMA((4, most)),
            pltpu.SemaphoreType.DMA((4, most)),
        ],
        compiler_params=pltpu.CompilerParams(
            collective_id=collective_id, has_side_effects=True, vmem_limit_bytes=VMEM_LIMIT
        ),
        name="reduce_group",
    )(partial, base)


def lanes_same(shape, row_width, column_width):
    return (
        lax.broadcasted_iota(jnp.int32, shape, 0) // row_width
        == lax.broadcasted_iota(jnp.int32, shape, 1) // column_width
    ).astype(F32)


def dot32(left, right, contract=((1,), (0,))):
    return lax.dot_general(
        left.astype(BF16), right.astype(BF16), (contract, ((), ())), preferred_element_type=F32
    )


def attend_rows(sums, shift, spike, scale, heads):
    length = sums.shape[0]
    key_lanes, value_lanes = heads * HEAD_K, heads * HEAD_V

    def part(start, width):
        return sums[:, start : start + width]

    def rounded(array):
        return array.astype(BF16).astype(F32)

    query = rounded(part(0, key_lanes)) * HEAD_K ** (-0.5)
    keys = rounded(part(key_lanes, key_lanes))
    values = rounded(part(2 * key_lanes, value_lanes))
    decay_pre = part(2 * key_lanes + value_lanes, key_lanes) + shift
    gate = rounded(part(3 * key_lanes + value_lanes, value_lanes))
    log_sigmoid = jnp.minimum(decay_pre, 0.0) - jnp.log1p(jnp.exp(-jnp.abs(decay_pre)))
    c = log_sigmoid / switch_multiplier + spike
    row = lax.broadcasted_iota(jnp.int32, (length, key_lanes), 0)
    step = 1
    while step < length:
        c = c + jnp.where(row >= step, pltpu.roll(c, step, 0), 0.0)
        step *= 2

    spread = lanes_same((key_lanes, value_lanes), HEAD_K, HEAD_V)
    in_sub = lax.rem(row, SUB)
    out = dot32(query * keys, spread) * values
    for d in range(1, SUB):
        ok = in_sub >= d
        weight = jnp.exp(jnp.where(ok, c - pltpu.roll(c, d, 0), 0.0))
        product = jnp.where(ok, query * pltpu.roll(keys, d, 0) * weight, 0.0)
        out = out + dot32(product, spread) * pltpu.roll(values, d, 0)

    pieces = [jnp.zeros((SUB, value_lanes), F32)]
    stack = heads * SUB
    key_mask = lanes_same((stack, key_lanes), SUB, HEAD_K)
    value_mask = lanes_same((stack, value_lanes), SUB, HEAD_V)
    for start in range(SUB, length, SUB):
        edge = c[start - 1 : start]
        q_part = query[start : start + SUB] * jnp.exp(c[start : start + SUB] - edge)
        k_part = keys[:start] * jnp.exp(edge - c[:start])
        stacked = jnp.concatenate([q_part] * heads, axis=0) * key_mask
        scores = dot32(stacked, k_part, ((1,), (1,)))
        read = dot32(scores, values[:start]) * value_mask
        total = read[:SUB]
        for h in range(1, heads):
            total = total + read[h * SUB : (h + 1) * SUB]
        pieces.append(total)
    out = out + jnp.concatenate(pieces, axis=0)

    same = lanes_same((value_lanes, value_lanes), HEAD_V, HEAD_V)
    mean = dot32(out * out, same) / HEAD_V
    out = out * lax.rsqrt(mean + norm_eps) * scale
    return (out * (gate / (1.0 + jnp.exp(-gate)))).astype(BF16)


def causal_conv(content_tokens, taps, length):
    rows, columns = content_tokens.shape
    content_tokens = content_tokens.astype(F32).reshape(rows // length, length, columns)
    taps = taps.astype(F32)
    width = taps.shape[0]
    padded = jnp.pad(content_tokens, ((0, 0), (width - 1, 0), (0, 0)))
    total = jnp.zeros_like(content_tokens)
    for offset in range(width):
        total = total + padded[:, offset : offset + length] * taps[offset]
    return total.reshape(rows, columns)


def pair_size(outer):
    return 2 if outer % 2 == 0 else 1


def fits(sizes, features, probe, result, content):
    n_rep, n_fs, n_tp = sizes
    outer, inner = factor(n_fs)
    members = n_rep * pair_size(outer)
    return (
        features.shape[0] % 16 == 0
        and features.shape[1] % 128 == 0
        and probe.shape[1] % (128 * n_rep) == 0
        and result.shape[1] % 128 == 0
        and result.shape[0] % (128 * n_rep) == 0
        and content.shape[1] % (128 * members) == 0
        and outer & (outer - 1) == 0
        and outer % n_tp == 0
    )


def partner(a, d, outer):
    total, bit = 0, 1
    while bit < outer:
        total = total + lax.rem(a // bit + (d // bit) % 2, 2) * bit
        bit *= 2
    return total


def shifted(array, step, row):
    return jnp.where(row >= step, pltpu.roll(array, step, 0), 0.0)


def taps_sum(array, taps):
    taps = taps.astype(F32)
    width = taps.shape[0]
    row = lax.broadcasted_iota(jnp.int32, array.shape, 0)
    total = jnp.zeros_like(array)
    for offset in range(width):
        back = width - 1 - offset
        moved = array if back == 0 else shifted(array, back, row)
        total = total + moved * taps[offset : offset + 1]
    return total


def whole_layer(
    sizes,
    features,
    first_gain,
    weights,
    shift,
    spike,
    scale,
    second_gain,
    content_taps,
    switch_taps,
):
    n_rep, n_fs, n_tp = sizes
    outer, inner = factor(n_fs)
    n_pair = pair_size(outer)
    members = n_rep * n_pair
    length, columns = features.shape
    wide = columns * n_tp
    rows = length * n_rep
    tokens = length * members
    key_lanes = weights[0].shape[1] // n_rep
    heads = key_lanes // HEAD_K
    value_lanes = heads * HEAD_V
    units = weights[6].shape[1] // members
    side = weights[5].shape[1]
    runs = outer // n_tp

    across = [weight.shape[0] for weight in weights[:5]] + [side]
    across += [weights[6].shape[0], weights[7].shape[0], side]
    kinds = ("project",) * 5 + ("result", "expand", "expand", "contract")
    widths = [weight.shape[1] // n_rep for weight in weights[:5]]
    offsets = [sum(widths[:w]) for w in range(5)]
    part_rows = {5: weights[5].shape[0] // n_rep, 8: weights[8].shape[0] // members}
    chunks = [(w, 0, weights[w].shape[0]) for w in range(5)] + [(5, 0, part_rows[5])]
    split = pieces_of(weights[6].shape[0], 2)
    size = weights[6].shape[0] // split
    chunks += [(w, k * size, size) for k in range(split) for w in (6, 7)]
    split = pieces_of(part_rows[8], 2)
    size = part_rows[8] // split
    chunks += [(8, k * size, size) for k in range(split)]
    count = len(chunks)

    def kernel(*refs):
        sources = refs[:9]
        (features_ref, gain_ref, shift_ref, spike_ref, scale_ref) = refs[9:14]
        (second_ref, content_taps_ref, switch_taps_ref, out_ref) = refs[14:18]
        (project_all, result_all, expand_all, contract_all) = refs[18:22]
        (whole_ref, normed_ref, spike_all, gated_ref, stage, slot_a, held, slot_b) = refs[22:30]
        (mid_all, normed_mid, hidden_ref, down_stage, slot_d, own_part, held_down, slot_c) = refs[
            30:38
        ]
        (far_send, far_recv, near_send, near_recv, own_sem) = refs[38:43]
        (group_send, group_recv, spike_send, spike_recv) = refs[43:47]
        (mix_send, mix_recv, cross_send, cross_recv) = refs[47:51]
        (mid_send, mid_recv, strip_send, strip_recv) = refs[51:55]
        (down_send, down_recv, back_send, back_recv) = refs[55:59]
        rep, fs, tp = lax.axis_index("rep"), lax.axis_index("fs"), lax.axis_index("tp")
        a, b = fs // inner, lax.rem(fs, inner)
        p = lax.rem(a, n_pair)
        far = [partner(a, d, outer) for d in range(1, outer)]
        near = [a * inner + lax.rem(b + d, inner) for d in range(1, inner)]
        tps = [lax.rem(tp + d, n_tp) for d in range(1, n_tp)]
        reps = [lax.rem(rep + d, n_rep) for d in range(1, n_rep)]
        group = [
            {"rep": lax.rem(rep + i, n_rep), "tp": lax.rem(tp + j, n_tp)}
            for i in range(n_rep)
            for j in range(n_tp)
            if i or j
        ]
        team = []
        senders = []
        diagonal = []
        for i in range(n_rep):
            for j in range(n_pair):
                if i or j:
                    r, q = lax.rem(rep + i, n_rep), lax.rem(p + j, n_pair)
                    peer = {"rep": r, "fs": (a - p + q) * inner + b}
                    team.append((peer, r * n_pair + q))
                    r, q = lax.rem(rep + n_rep - i, n_rep), lax.rem(p + n_pair - j, n_pair)
                    senders.append(r * n_pair + q)
                    if i and j:
                        diagonal.append(peer)
        me = rep * n_pair + p
        greeted = [{"fs": index * inner + b} for index in far]
        greeted += [{"fs": index} for index in near] + group + diagonal
        barrier = pltpu.get_barrier_semaphore()
        for peer in greeted:
            pl.semaphore_signal(barrier, inc=1, device_id=peer, device_id_type=MESH)
        pl.semaphore_wait(barrier, len(greeted))

        def at(start, size):
            return pl.ds(pl.multiple_of(start, size), size)

        def source(c, position):
            w, start, size = chunks[c]
            member = rep * n_pair + lax.rem(position, n_pair)
            if kinds[w] == "project":
                return sources[w].at[pl.ds(start, size), at(rep * widths[w], widths[w])]
            if kinds[w] == "expand":
                return sources[w].at[pl.ds(start, size), at(member * units, units)]
            index = rep if kinds[w] == "result" else member
            base = pl.multiple_of(index * part_rows[w], part_rows[w])
            return sources[w].at[pl.ds(base + start, size), :]

        def block(c, index):
            w, start, size = chunks[c]
            base = pl.multiple_of(index * across[w], across[w])
            if kinds[w] == "project":
                return project_all.at[pl.ds(base + start, size), pl.ds(offsets[w], widths[w])]
            if kinds[w] == "expand":
                return expand_all.at[pl.ds(base + start, size), pl.ds((w - 6) * units, units)]
            target = result_all if kinds[w] == "result" else contract_all
            return target.at[pl.ds(start, size), pl.ds(base, across[w])]

        sent = []
        far_copies, near_copies, own_copies = {}, {}, {}

        def launch_far(c):
            far_copies[c] = [
                send_to(
                    source(c, position),
                    block(c, fs),
                    far_send.at[c, d],
                    far_recv.at[c, d],
                    {"fs": position * inner + b},
                )
                for d, position in enumerate(far)
            ]
            sent.extend(far_copies[c])

        def launch_near(c):
            near_copies[c] = [
                send_to(
                    source(c, a),
                    block(c, fs),
                    near_send.at[c, 0, e],
                    near_recv.at[c, 0, e],
                    {"fs": index},
                )
                for e, index in enumerate(near)
            ]
            sent.extend(near_copies[c])
            own_copies[c] = pltpu.make_async_copy(source(c, a), block(c, fs), own_sem.at[c])
            own_copies[c].start()

        def forward(c):
            for d, position in enumerate(far):
                far_copies[c][d].wait_recv()
                landed = block(c, position * inner + b)
                copies = [
                    send_to(
                        landed,
                        landed,
                        near_send.at[c, d + 1, e],
                        near_recv.at[c, d + 1, e],
                        {"fs": index},
                    )
                    for e, index in enumerate(near)
                ]
                near_copies[c] += copies
                sent.extend(copies)

        def arrived(c):
            for copy in near_copies[c]:
                copy.wait_recv()
            own_copies[c].wait()

        first = [c for c in range(count) if kinds[chunks[c][0]] == "project"]
        second = [c for c in range(count) if kinds[chunks[c][0]] == "result"]
        third = [c for c in range(count) if kinds[chunks[c][0]] == "expand"]
        fourth = [c for c in range(count) if kinds[chunks[c][0]] == "contract"]

        spot = whole_ref.at[at(rep * length, length), at(tp * columns, columns)]
        own_features = pltpu.make_async_copy(features_ref, spot, own_sem.at[count])
        own_features.start()
        group_copies = [
            send_to(features_ref, spot, group_send.at[d], group_recv.at[d], peer)
            for d, peer in enumerate(group)
        ]
        lines = spike_all.at[at(rep * length, length), :]
        own_spike = pltpu.make_async_copy(
            spike_ref.at[:, at(rep * key_lanes, key_lanes)], lines, own_sem.at[count + 1]
        )
        own_spike.start()
        group_copies += [
            send_to(
                spike_ref.at[:, at(index * key_lanes, key_lanes)],
                lines,
                spike_send.at[d],
                spike_recv.at[d],
                {"rep": index},
            )
            for d, index in enumerate(reps)
        ]
        for c in first:
            launch_far(c)
            launch_near(c)
        for c in second + third:
            launch_far(c)
        own_features.wait()
        own_spike.wait()
        for copy in group_copies:
            copy.wait()

        def first_norm(i, carry):
            lines = at(i * length, length)
            normed_ref[lines, :] = row_norm(whole_ref[lines, :], gain_ref[...])
            return carry

        lax.fori_loop(0, n_rep, first_norm, 0)
        for c in first:
            forward(c)
        half = len(third) // 2
        for c in second + third[:half]:
            launch_near(c)
        for c in first:
            arrived(c)

        def attention(index):
            lines = at(index * length, length)
            sums = jnp.dot(normed_ref[lines, :], project_all[...], preferred_element_type=F32)
            gated_ref[lines, :] = attend_rows(
                sums,
                shift_ref[:, at(rep * key_lanes, key_lanes)],
                spike_all[lines, :],
                scale_ref[:, at(rep * value_lanes, value_lanes)].astype(F32),
                heads,
            )

        order = reps + [rep]
        attention(order[0])
        for c in second:
            forward(c)
        for c in third[half:]:
            launch_near(c)
        for index in order[1:]:
            attention(index)
        for c in third[:half]:
            forward(c)
        for c in second:
            arrived(c)

        def mixed(index, strip):
            return jnp.dot(
                gated_ref[at(index * length, length), :],
                result_all[:, at(strip * columns, columns)],
                preferred_element_type=F32,
            )

        mix_copies = []
        for i, index in enumerate(order):
            copies = []
            for d, other in enumerate(tps):
                stage[i, d] = mixed(index, other).astype(BF16)
                copies.append(
                    send_to(
                        stage.at[i, d],
                        slot_a.at[i, d],
                        mix_send.at[i, d],
                        mix_recv.at[i, d],
                        {"tp": other},
                    )
                )
            mix_copies.append(copies)
            sent.extend(copies)
        cross_copies = []
        for i, index in enumerate(order):
            total = mixed(index, tp)
            for d, copy in enumerate(mix_copies[i]):
                copy.wait_recv()
                total = total + slot_a[i, d].astype(F32)
            if i < n_rep - 1:
                held[i] = total.astype(BF16)
                copy = send_to(
                    held.at[i],
                    slot_b.at[i],
                    cross_send.at[i],
                    cross_recv.at[i],
                    {"rep": index},
                )
                cross_copies.append(copy)
                sent.append(copy)
            else:
                for d, copy in enumerate(cross_copies):
                    copy.wait_recv()
                    total = total + slot_b[d].astype(F32)
        base = whole_ref[at(rep * length, length), at(tp * columns, columns)].astype(F32)
        mine = mid_all.at[at(me * length, length), at(tp * columns, columns)]
        mine[...] = (base + total.astype(BF16).astype(F32)).astype(BF16)

        mid_copies = [
            send_to(mine, mine, mid_send.at[k], mid_recv.at[k], peer)
            for k, (peer, member) in enumerate(team)
        ]
        sent.extend(mid_copies)
        strip_copies = []

        def strips(k, member):
            strip = mid_all.at[at(member * length, length), at(tp * columns, columns)]
            copies = [
                send_to(
                    strip, strip, strip_send.at[k, d], strip_recv.at[k, d], {"tp": index}
                )
                for d, index in enumerate(tps)
            ]
            strip_copies.append(copies)
            sent.extend(copies)

        strips(0, me)
        for c in fourth:
            launch_far(c)
        for c in third[half:]:
            forward(c)
        for c in fourth:
            launch_near(c)
        for k, member in enumerate(senders):
            mid_copies[k].wait_recv()
            strips(k + 1, member)

        def second_norm(member):
            lines = at(member * length, length)
            normed_mid[lines, :] = row_norm(mid_all[lines, :], second_ref[...])

        for k, member in enumerate([me] + senders):
            for copy in strip_copies[k]:
                copy.wait_recv()
            second_norm(member)
        for c in third:
            arrived(c)

        def expand(i, carry):
            lines = at(i * length, length)
            both = jnp.dot(normed_mid[lines, :], expand_all[...], preferred_element_type=F32)
            both = both.astype(BF16).astype(F32)
            value = taps_sum(both[:, :units], content_taps_ref[:, at(me * units, units)])
            gate = taps_sum(both[:, units:], switch_taps_ref[:, at(me * units, units)])
            hidden_ref[lines, :] = (value * jax.nn.gelu(gate, approximate=True)).astype(BF16)
            return carry

        lax.fori_loop(0, members, expand, 0)
        for c in fourth:
            forward(c)

        back_copies = []
        for e in range(inner):
            lane = lax.rem(b + inner - e, inner)
            for c in fourth:
                if e == 0:
                    own_copies[c].wait()
                else:
                    for d in range(outer):
                        near_copies[c][d * (inner - 1) + e - 1].wait_recv()
            spots = [at((run * inner + lane) * side, side) for run in range(runs)]

            def product(strip, run):
                index = (strip * runs + run) * inner + lane
                return jnp.dot(
                    hidden_ref[...],
                    contract_all[:, at(index * side, side)],
                    preferred_element_type=F32,
                )

            down_copies = []
            for run in range(runs):
                copies = []
                for d, other in enumerate(tps):
                    down_stage[d, :, spots[run]] = product(other, run).astype(BF16)
                    copies.append(
                        send_to(
                            down_stage.at[d, :, spots[run]],
                            slot_d.at[d, :, spots[run]],
                            down_send.at[e, run, d],
                            down_recv.at[e, run, d],
                            {"tp": other},
                        )
                    )
                down_copies.append(copies)
                sent.extend(copies)
            for run in range(runs):
                total = product(tp, run)
                for d, copy in enumerate(down_copies[run]):
                    copy.wait_recv()
                    total = total + slot_d[d, :, spots[run]].astype(F32)
                own_part[:, spots[run]] = total
                held_down[:, spots[run]] = total.astype(BF16)
                for k, (peer, member) in enumerate(team):
                    copy = send_to(
                        held_down.at[at(member * length, length), spots[run]],
                        slot_c.at[k, :, spots[run]],
                        back_send.at[e, run, k],
                        back_recv.at[e, run, k],
                        peer,
                    )
                    back_copies.append(copy)
        for copy in back_copies:
            copy.wait_recv()
        total = own_part[at(me * length, length), :]
        for k in range(members - 1):
            total = total + slot_c[k].astype(F32)
        out_ref[...] = (mine[...].astype(F32) + total.astype(BF16).astype(F32)).astype(BF16)
        for copy in sent + back_copies:
            copy.wait_send()

    dma = pltpu.SemaphoreType.DMA
    vmem = pl.BlockSpec(memory_space=pltpu.VMEM)
    hbm = pl.BlockSpec(memory_space=pl.ANY)

    def pair(*shape):
        shape = tuple(max(n, 1) for n in shape)
        return [dma(shape), dma(shape)]

    def room(*shape, dtype=BF16):
        return pltpu.VMEM(tuple(max(n, 1) for n in shape), dtype)

    depth = weights[0].shape[0] * n_fs
    scratch = [
        room(depth, sum(widths)),
        room(part_rows[5], side * n_fs),
        room(depth, 2 * units),
        room(part_rows[8], side * n_fs),
        room(rows, wide),
        room(rows, wide),
        room(rows, key_lanes, dtype=F32),
        room(rows, value_lanes),
        room(n_rep, n_tp - 1, length, columns),
        room(n_rep, n_tp - 1, length, columns),
        room(n_rep - 1, length, columns),
        room(n_rep - 1, length, columns),
        room(tokens, wide),
        room(tokens, wide),
        room(tokens, units),
        room(n_tp - 1, tokens, columns),
        room(n_tp - 1, tokens, columns),
        room(tokens, columns, dtype=F32),
        room(tokens, columns),
        room(members - 1, length, columns),
    ]
    scratch += pair(count, outer - 1) + pair(count, outer, inner - 1) + [dma((count + 2,))]
    scratch += pair(n_rep * n_tp - 1) + pair(n_rep - 1)
    scratch += pair(n_rep, n_tp - 1) + pair(n_rep - 1)
    scratch += pair(members - 1) + pair(members, n_tp - 1)
    scratch += pair(inner, runs, n_tp - 1) + pair(inner, runs, members - 1)
    return pl.pallas_call(
        kernel,
        out_shape=jax.ShapeDtypeStruct((length, columns), BF16),
        in_specs=[hbm] * 10 + [vmem] * 7,
        out_specs=vmem,
        scratch_shapes=scratch,
        compiler_params=pltpu.CompilerParams(
            collective_id=0, has_side_effects=True, vmem_limit_bytes=VMEM_LIMIT
        ),
        name="whole_layer",
    )(
        *weights,
        features,
        first_gain.reshape(1, -1),
        shift.reshape(1, -1),
        spike,
        scale.reshape(1, -1),
        second_gain.reshape(1, -1),
        content_taps,
        switch_taps,
    )


def shards(
    sizes,
    incoming_features,
    attend_prenormal_scale,
    probe_matrix,
    lookup_matrix,
    content_matrix,
    forgetting_matrix,
    result_switch_matrix,
    forgetting_shift,
    spike_forget_logarithm,
    attend_unit_scale,
    attend_result_matrix,
    perceptron_scale,
    content_expand_matrix,
    switch_expand_matrix,
    content_kernel,
    switch_kernel,
    contract_matrix,
):
    n_rep, n_fs, n_tp = sizes
    rep = lax.axis_index("rep")
    length = incoming_features.shape[0]
    if fits(
        sizes, incoming_features, probe_matrix, attend_result_matrix, content_expand_matrix
    ):
        return whole_layer(
            sizes,
            incoming_features,
            attend_prenormal_scale,
            (
                probe_matrix,
                lookup_matrix,
                content_matrix,
                forgetting_matrix,
                result_switch_matrix,
                attend_result_matrix,
                content_expand_matrix,
                switch_expand_matrix,
                contract_matrix,
            ),
            forgetting_shift,
            spike_forget_logarithm,
            attend_unit_scale,
            perceptron_scale,
            content_kernel,
            switch_kernel,
        )

    def mine(array, axis):
        size = array.shape[axis] // n_rep
        return lax.dynamic_slice_in_dim(array, rep * size, size, axis)

    project = jnp.concatenate(
        [
            mine(matrix, 1)
            for matrix in (
                probe_matrix,
                lookup_matrix,
                content_matrix,
                forgetting_matrix,
                result_switch_matrix,
            )
        ],
        axis=1,
    )
    spike_all = lax.all_to_all(
        spike_forget_logarithm, "rep", split_axis=1, concat_axis=0, tiled=True
    )
    expand = jnp.concatenate([mine(content_expand_matrix, 1), mine(switch_expand_matrix, 1)], axis=1)
    side = attend_result_matrix.shape[1]
    inside = side % 128 == 0
    outs = first_half(
        project,
        mine(attend_result_matrix, 0),
        expand,
        mine(contract_matrix, 0),
        incoming_features,
        attend_prenormal_scale,
        mine(forgetting_shift, 0),
        spike_all,
        mine(attend_unit_scale, 0),
        1 if inside else 0,
        inside,
        sizes,
    )
    if inside:
        expand_all, contract_all, middle, whole_mid = outs
    else:
        expand_all, contract_all, result_all, switched_result = outs
        result_all, contract_all = (
            array.reshape(n_fs, -1, side).swapaxes(0, 1).reshape(-1, n_fs * side)
            for array in (result_all, contract_all)
        )
        mixer_partial = jnp.dot(switched_result, result_all, preferred_element_type=F32)
        middle, whole_mid = reduce_group(
            mixer_partial.astype(BF16), incoming_features, sizes, True, 2
        )
    normed_mid = row_norm(whole_mid, perceptron_scale)
    both = jnp.dot(normed_mid, expand_all, preferred_element_type=F32).astype(BF16)
    half = both.shape[1] // 2
    conv_value = causal_conv(both[:, :half], mine(content_kernel, 1), length)
    conv_gated = causal_conv(both[:, half:], mine(switch_kernel, 1), length)
    hidden = (conv_value * jax.nn.gelu(conv_gated, approximate=True)).astype(BF16)
    down_partial = jnp.dot(hidden, contract_all, preferred_element_type=F32).astype(BF16)
    return reduce_group(down_partial, middle, sizes, False, 3)[0]


def solution(mesh):
    sizes = (mesh.shape["rep"], mesh.shape["fs"], mesh.shape["tp"])
    placed = (
        P(("rep", "fs"), "tp"),
        P(),
        P("fs", "tp"),
        P("fs", "tp"),
        P("fs", "tp"),
        P("fs", "tp"),
        P("fs", "tp"),
        P("tp"),
        P(("rep", "fs"), "tp"),
        P("tp"),
        P("tp", "fs"),
        P(),
        P("fs", "tp"),
        P("fs", "tp"),
        P(None, "tp"),
        P(None, "tp"),
        P("tp", "fs"),
    )
    return jax.shard_map(
        functools.partial(shards, sizes),
        mesh=mesh,
        in_specs=placed,
        out_specs=P(("rep", "fs"), "tp"),
        check_vma=False,
    )
```

```python
import functools

import jax
import jax.numpy as jnp
from jax import lax
from jax.experimental import pallas as pl
from jax.experimental.pallas import tpu as pltpu
from jax.sharding import PartitionSpec as P

HEAD_K = 32
HEAD_V = 64
SUB = 16

norm_eps = 1e-06
switch_multiplier = 16.0
MESH = pl.DeviceIdType.MESH
F32 = jnp.float32
BF16 = jnp.bfloat16
VMEM_LIMIT = 60 * 1024 * 1024


def row_norm(content_tokens, gain):
    content_tokens = content_tokens.astype(F32)
    scaled = content_tokens * lax.rsqrt(
        jnp.mean(content_tokens * content_tokens, axis=-1, keepdims=True) + norm_eps
    )
    return (scaled * gain.astype(F32)).astype(BF16)


def factor(n):
    inner = 1
    for size in range(1, n + 1):
        if n % size == 0 and size * size <= n:
            inner = size
    return n // inner, inner


def place(ref, axis, index, size):
    at = pl.ds(pl.multiple_of(index * size, size), size)
    return ref.at[at, :] if axis == 0 else ref.at[:, at]


def send_to(source, target, send_sem, recv_sem, peer):
    copy = pltpu.make_async_remote_copy(
        src_ref=source,
        dst_ref=target,
        send_sem=send_sem,
        recv_sem=recv_sem,
        device_id=peer,
        device_id_type=MESH,
    )
    copy.start()
    return copy


def pieces_of(rows, most):
    for count in range(most, 1, -1):
        if rows % (16 * count) == 0:
            return count
    return 1


def first_half(
    project, result, expand, contract, features, gain, shift, spike, scale, axis, inside, sizes
):
    n_rep, n_fs, n_tp = sizes
    outer, inner = factor(n_fs)
    length, columns = features.shape
    rows = length * n_rep
    heads = shift.shape[0] // HEAD_K
    value_lanes = heads * HEAD_V
    group = n_rep * n_tp
    most = max(n_rep, n_tp)
    weights = (project, result, expand, contract)
    axes = (0, axis, 0, axis)
    splits = (2, 1, 4, 4)
    full = []
    chunks = []
    for w in range(4):
        shape = list(weights[w].shape)
        size = shape[0]
        shape[axes[w]] *= n_fs
        full.append(tuple(shape))
        split = pieces_of(size, splits[w])
        chunks += [(w, k * (size // split), size // split) for k in range(split)]
    count = len(chunks)

    def kernel(*refs):
        sources = refs[:4]
        features_ref, gain_ref, shift_ref, spike_ref, scale_ref = refs[4:9]
        if inside:
            expand_out, contract_out, middle_ref, mid_ref = refs[9:13]
            rest = refs[13:]
            result_out, gated_ref, partial_ref, slot_a, held, slot_b = rest[:6]
            rest = rest[6:]
        else:
            expand_out, contract_out, result_out, gated_ref = refs[9:13]
            rest = refs[13:]
        project_out, whole_ref = rest[:2]
        far_send, far_recv, near_send, near_recv, own_sem, group_send, group_recv = rest[2:9]
        if inside:
            sum_send, sum_recv = rest[9:]
        outs = (project_out, result_out, expand_out, contract_out)
        rep, fs, tp = lax.axis_index("rep"), lax.axis_index("fs"), lax.axis_index("tp")
        a, b = fs // inner, lax.rem(fs, inner)
        far = [lax.rem(a + d, outer) * inner + b for d in range(1, outer)]
        near = [a * inner + lax.rem(b + d, inner) for d in range(1, inner)]
        peers = [{"fs": index} for index in far + near]
        others = [
            {"rep": lax.rem(rep + i, n_rep), "tp": lax.rem(tp + j, n_tp)}
            for i in range(n_rep)
            for j in range(n_tp)
            if i or j
        ]
        barrier = pltpu.get_barrier_semaphore()
        for peer in peers + others:
            pl.semaphore_signal(barrier, inc=1, device_id=peer, device_id_type=MESH)
        pl.semaphore_wait(barrier, len(peers) + len(others))

        def block(w, start, size, index):
            across = weights[w].shape[axes[w]]
            offset = pl.multiple_of(index * across, across)
            if axes[w] == 0:
                return outs[w].at[pl.ds(offset + start, size), :]
            return outs[w].at[pl.ds(start, size), pl.ds(offset, across)]

        far_copies, near_copies, own_copies = {}, {}, {}

        def launch_far(c):
            w, start, size = chunks[c]
            source, target = sources[w].at[pl.ds(start, size), :], block(w, start, size, fs)
            far_copies[c] = [
                send_to(source, target, far_send.at[c, d], far_recv.at[c, d], {"fs": index})
                for d, index in enumerate(far)
            ]

        def launch_near(c):
            w, start, size = chunks[c]
            source, target = sources[w].at[pl.ds(start, size), :], block(w, start, size, fs)
            near_copies[c] = [
                send_to(
                    source, target, near_send.at[c, 0, e], near_recv.at[c, 0, e], {"fs": index}
                )
                for e, index in enumerate(near)
            ]
            own_copies[c] = pltpu.make_async_copy(source, target, own_sem.at[c])
            own_copies[c].start()

        def forward(c):
            w, start, size = chunks[c]
            for d in range(1, outer):
                far_copies[c][d - 1].wait_recv()
                held_block = block(w, start, size, lax.rem(a + outer - d, outer) * inner + b)
                near_copies[c] += [
                    send_to(
                        held_block,
                        held_block,
                        near_send.at[c, d, e],
                        near_recv.at[c, d, e],
                        {"fs": index},
                    )
                    for e, index in enumerate(near)
                ]

        def arrived(c):
            for copy in near_copies[c]:
                copy.wait_recv()
            own_copies[c].wait()

        first = [c for c in range(count) if chunks[c][0] == 0]
        second = [c for c in range(count) if chunks[c][0] == 1]
        later = [c for c in range(count) if chunks[c][0] > 1]

        spot = whole_ref.at[
            pl.ds(pl.multiple_of(rep * length, length), length),
            pl.ds(pl.multiple_of(tp * columns, columns), columns),
        ]
        own = pltpu.make_async_copy(features_ref, spot, own_sem.at[count])
        own.start()
        group_copies = [
            send_to(features_ref, spot, group_send.at[d], group_recv.at[d], peer)
            for d, peer in enumerate(others)
        ]
        for c in first:
            launch_far(c)
            launch_near(c)
        for c in second + later:
            launch_far(c)
        for c in first:
            forward(c)
        for c in second + later:
            launch_near(c)
        for c in first:
            arrived(c)
        own.wait()
        for copy in group_copies:
            copy.wait()

        def sequence(i, carry):
            at = pl.ds(pl.multiple_of(i * length, length), length)
            normed = row_norm(whole_ref[at, :], gain_ref[...])
            sums = jnp.dot(normed, project_out[...], preferred_element_type=F32)
            gated_ref[at, :] = attend_rows(
                sums, shift_ref[...], spike_ref[at, :], scale_ref[...], heads
            )
            return carry

        lax.fori_loop(0, n_rep, sequence, 0)
        for c in second:
            forward(c)
        waiting = list(later)
        for c in waiting[:1]:
            forward(c)
        waiting = waiting[1:]
        for c in second:
            arrived(c)
        if inside:

            def mixer(i, carry):
                at = pl.ds(pl.multiple_of(i * length, length), length)
                partial_ref[at, :] = jnp.dot(
                    gated_ref[at, :], result_out[...], preferred_element_type=F32
                ).astype(BF16)
                return carry

            lax.fori_loop(0, n_rep, mixer, 0)

            def between(stage):
                if stage in (1, 2):
                    forward(waiting.pop(0))

            reduce_steps(
                partial_ref,
                features_ref,
                middle_ref,
                mid_ref,
                slot_a,
                held,
                slot_b,
                sum_send,
                sum_recv,
                sizes,
                between,
            )
        for c in waiting:
            forward(c)
        for c in later:
            arrived(c)
        for c in range(count):
            for copy in far_copies[c] + near_copies[c]:
                copy.wait_send()

    dma = pltpu.SemaphoreType.DMA
    vmem = pl.BlockSpec(memory_space=pltpu.VMEM)
    hbm = pl.BlockSpec(memory_space=pl.ANY)
    out_shape = [jax.ShapeDtypeStruct(full[2], BF16), jax.ShapeDtypeStruct(full[3], BF16)]
    scratch = []
    gated_shape = (rows, value_lanes)
    if inside:
        out_shape += [
            jax.ShapeDtypeStruct((length, columns), BF16),
            jax.ShapeDtypeStruct((rows, columns * n_tp), BF16),
        ]
        out_specs = [hbm, hbm, vmem, vmem]
        scratch += [
            pltpu.VMEM(full[1], BF16),
            pltpu.VMEM(gated_shape, BF16),
            pltpu.VMEM((rows, columns * n_tp), BF16),
            pltpu.VMEM((max(n_tp - 1, 1), rows, columns), BF16),
            pltpu.VMEM((rows, columns), BF16),
            pltpu.VMEM((max(n_rep - 1, 1), length, columns), BF16),
        ]
    else:
        out_shape += [
            jax.ShapeDtypeStruct(full[1], BF16),
            jax.ShapeDtypeStruct(gated_shape, BF16),
        ]
        out_specs = [hbm, hbm, hbm, vmem]
    scratch += [
        pltpu.VMEM(full[0], BF16),
        pltpu.VMEM((rows, columns * n_tp), BF16),
        dma((count, max(outer - 1, 1))),
        dma((count, max(outer - 1, 1))),
        dma((count, outer, max(inner - 1, 1))),
        dma((count, outer, max(inner - 1, 1))),
        dma((count + 1,)),
        dma((group,)),
        dma((group,)),
    ]
    if inside:
        scratch += [dma((4, most)), dma((4, most))]
    return pl.pallas_call(
        kernel,
        out_shape=out_shape,
        in_specs=[vmem] * 9,
        out_specs=out_specs,
        scratch_shapes=scratch,
        compiler_params=pltpu.CompilerParams(
            collective_id=0, has_side_effects=True, vmem_limit_bytes=VMEM_LIMIT
        ),
        name="first_half",
    )(
        *weights,
        features,
        gain.reshape(1, -1),
        shift.reshape(1, -1),
        spike,
        scale.astype(F32).reshape(1, -1),
    )


def reduce_steps(
    part_ref, base_ref, out_ref, all_ref, slot_a, held, slot_b, send_sem, recv_sem, sizes, between
):
    n_rep, n_fs, n_tp = sizes
    rows, columns = base_ref.shape
    rep, tp = lax.axis_index("rep"), lax.axis_index("tp")
    tps = [lax.rem(tp + d, n_tp) for d in range(1, n_tp)]
    reps = [lax.rem(rep + d, n_rep) for d in range(1, n_rep)]

    def send(stage, d, source, target, peer):
        return send_to(source, target, send_sem.at[stage, d], recv_sem.at[stage, d], peer)

    copies = [
        send(0, d, place(part_ref, 1, index, columns), slot_a.at[d], {"tp": index})
        for d, index in enumerate(tps)
    ]
    for copy in copies:
        copy.wait()
    total = place(part_ref, 1, tp, columns)[...].astype(F32)
    for d in range(len(tps)):
        total = total + slot_a[d].astype(F32)
    held[...] = total.astype(BF16)
    copies = [
        send(1, d, place(held, 0, index, rows), slot_b.at[d], {"rep": index})
        for d, index in enumerate(reps)
    ]
    between(1)
    for copy in copies:
        copy.wait()
    total = place(held, 0, rep, rows)[...].astype(F32)
    for d in range(len(reps)):
        total = total + slot_b[d].astype(F32)
    result = (base_ref[...].astype(F32) + total.astype(BF16).astype(F32)).astype(BF16)
    out_ref[...] = result
    if all_ref is not None:
        block = all_ref.at[
            pl.ds(pl.multiple_of(rep * rows, rows), rows),
            pl.ds(pl.multiple_of(tp * columns, columns), columns),
        ]
        block[...] = result
        copies = [send(2, d, block, block, {"rep": index}) for d, index in enumerate(reps)]
        between(2)
        for copy in copies:
            copy.wait()
        strip = place(all_ref, 1, tp, columns)
        copies = [send(3, d, strip, strip, {"tp": index}) for d, index in enumerate(tps)]
        for copy in copies:
            copy.wait()


def reduce_group(partial, base, sizes, spread, collective_id):
    n_rep, n_fs, n_tp = sizes
    rows, columns = base.shape

    def kernel(*refs):
        part_ref, base_ref = refs[:2]
        if spread:
            out_ref, all_ref, slot_a, held, slot_b, send_sem, recv_sem = refs[2:]
        else:
            all_ref = None
            out_ref, slot_a, held, slot_b, send_sem, recv_sem = refs[2:]
        rep, tp = lax.axis_index("rep"), lax.axis_index("tp")
        barrier = pltpu.get_barrier_semaphore()
        for d in range(1, n_tp):
            peer = {"tp": lax.rem(tp + d, n_tp)}
            pl.semaphore_signal(barrier, inc=1, device_id=peer, device_id_type=MESH)
        for d in range(1, n_rep):
            peer = {"rep": lax.rem(rep + d, n_rep)}
            pl.semaphore_signal(barrier, inc=1, device_id=peer, device_id_type=MESH)
        pl.semaphore_wait(barrier, n_tp + n_rep - 2)
        reduce_steps(
            part_ref,
            base_ref,
            out_ref,
            all_ref,
            slot_a,
            held,
            slot_b,
            send_sem,
            recv_sem,
            sizes,
            lambda stage: None,
        )

    out_shape = [jax.ShapeDtypeStruct((rows, columns), BF16)]
    if spread:
        out_shape.append(jax.ShapeDtypeStruct((rows * n_rep, columns * n_tp), BF16))
    vmem = pl.BlockSpec(memory_space=pltpu.VMEM)
    most = max(n_rep, n_tp)
    return pl.pallas_call(
        kernel,
        out_shape=out_shape,
        in_specs=[vmem, vmem],
        out_specs=[vmem] * len(out_shape),
        scratch_shapes=[
            pltpu.VMEM((max(n_tp - 1, 1), rows * n_rep, columns), BF16),
            pltpu.VMEM((rows * n_rep, columns), BF16),
            pltpu.VMEM((max(n_rep - 1, 1), rows, columns), BF16),
            pltpu.SemaphoreType.DMA((4, most)),
            pltpu.SemaphoreType.DMA((4, most)),
        ],
        compiler_params=pltpu.CompilerParams(
            collective_id=collective_id, has_side_effects=True, vmem_limit_bytes=VMEM_LIMIT
        ),
        name="reduce_group",
    )(partial, base)


def lanes_same(shape, row_width, column_width):
    return (
        lax.broadcasted_iota(jnp.int32, shape, 0) // row_width
        == lax.broadcasted_iota(jnp.int32, shape, 1) // column_width
    ).astype(F32)


def dot32(left, right, contract=((1,), (0,))):
    return lax.dot_general(
        left.astype(BF16), right.astype(BF16), (contract, ((), ())), preferred_element_type=F32
    )


def attend_rows(sums, shift, spike, scale, heads):
    length = sums.shape[0]
    key_lanes, value_lanes = heads * HEAD_K, heads * HEAD_V

    def part(start, width):
        return sums[:, start : start + width]

    def rounded(array):
        return array.astype(BF16).astype(F32)

    query = rounded(part(0, key_lanes)) * HEAD_K ** (-0.5)
    keys = rounded(part(key_lanes, key_lanes))
    values = rounded(part(2 * key_lanes, value_lanes))
    decay_pre = part(2 * key_lanes + value_lanes, key_lanes) + shift
    gate = rounded(part(3 * key_lanes + value_lanes, value_lanes))
    log_sigmoid = jnp.minimum(decay_pre, 0.0) - jnp.log1p(jnp.exp(-jnp.abs(decay_pre)))
    c = log_sigmoid / switch_multiplier + spike
    row = lax.broadcasted_iota(jnp.int32, (length, key_lanes), 0)
    step = 1
    while step < length:
        c = c + jnp.where(row >= step, pltpu.roll(c, step, 0), 0.0)
        step *= 2

    spread = lanes_same((key_lanes, value_lanes), HEAD_K, HEAD_V)
    in_sub = lax.rem(row, SUB)
    out = dot32(query * keys, spread) * values
    for d in range(1, SUB):
        ok = in_sub >= d
        weight = jnp.exp(jnp.where(ok, c - pltpu.roll(c, d, 0), 0.0))
        product = jnp.where(ok, query * pltpu.roll(keys, d, 0) * weight, 0.0)
        out = out + dot32(product, spread) * pltpu.roll(values, d, 0)

    pieces = [jnp.zeros((SUB, value_lanes), F32)]
    stack = heads * SUB
    key_mask = lanes_same((stack, key_lanes), SUB, HEAD_K)
    value_mask = lanes_same((stack, value_lanes), SUB, HEAD_V)
    for start in range(SUB, length, SUB):
        edge = c[start - 1 : start]
        q_part = query[start : start + SUB] * jnp.exp(c[start : start + SUB] - edge)
        k_part = keys[:start] * jnp.exp(edge - c[:start])
        stacked = jnp.concatenate([q_part] * heads, axis=0) * key_mask
        scores = dot32(stacked, k_part, ((1,), (1,)))
        read = dot32(scores, values[:start]) * value_mask
        total = read[:SUB]
        for h in range(1, heads):
            total = total + read[h * SUB : (h + 1) * SUB]
        pieces.append(total)
    out = out + jnp.concatenate(pieces, axis=0)

    same = lanes_same((value_lanes, value_lanes), HEAD_V, HEAD_V)
    mean = dot32(out * out, same) / HEAD_V
    out = out * lax.rsqrt(mean + norm_eps) * scale
    return (out * (gate / (1.0 + jnp.exp(-gate)))).astype(BF16)


def causal_conv(content_tokens, taps, length):
    rows, columns = content_tokens.shape
    content_tokens = content_tokens.astype(F32).reshape(rows // length, length, columns)
    taps = taps.astype(F32)
    width = taps.shape[0]
    padded = jnp.pad(content_tokens, ((0, 0), (width - 1, 0), (0, 0)))
    total = jnp.zeros_like(content_tokens)
    for offset in range(width):
        total = total + padded[:, offset : offset + length] * taps[offset]
    return total.reshape(rows, columns)


def pair_size(outer):
    return 2 if outer % 2 == 0 else 1


def fits(sizes, features, probe, result, content):
    n_rep, n_fs, n_tp = sizes
    outer, inner = factor(n_fs)
    members = n_rep * pair_size(outer)
    return (
        features.shape[0] % 16 == 0
        and features.shape[1] % 128 == 0
        and probe.shape[0] % (16 * n_rep) == 0
        and probe.shape[1] % (128 * inner) == 0
        and result.shape[1] % 128 == 0
        and result.shape[0] % (128 * inner * n_rep) == 0
        and content.shape[1] % (128 * members) == 0
        and outer & (outer - 1) == 0
        and members == 2 * n_rep
        and outer % n_tp == 0
    )


def partner(a, d, outer):
    total, bit = 0, 1
    while bit < outer:
        total = total + lax.rem(a // bit + (d // bit) % 2, 2) * bit
        bit *= 2
    return total


def shifted(array, step, row):
    return jnp.where(row >= step, pltpu.roll(array, step, 0), 0.0)


def taps_sum(array, taps):
    taps = taps.astype(F32)
    width = taps.shape[0]
    row = lax.broadcasted_iota(jnp.int32, array.shape, 0)
    total = jnp.zeros_like(array)
    for offset in range(width):
        back = width - 1 - offset
        moved = array if back == 0 else shifted(array, back, row)
        total = total + moved * taps[offset : offset + 1]
    return total


def whole_layer(
    sizes,
    features,
    first_gain,
    weights,
    shift,
    spike,
    scale,
    second_gain,
    content_taps,
    switch_taps,
):
    n_rep, n_fs, n_tp = sizes
    outer, inner = factor(n_fs)
    n_pair = pair_size(outer)
    members = n_rep * n_pair
    length, columns = features.shape
    wide = columns * n_tp
    rows = length * inner
    tokens = length * members
    key_lanes = weights[0].shape[1] // inner
    heads = key_lanes // HEAD_K
    value_lanes = heads * HEAD_V
    units = weights[6].shape[1] // members
    side = weights[5].shape[1]
    runs = outer // n_tp
    aligned = runs == n_pair
    pieces = pieces_of(length, 2)

    firsts = (0, 1, 3, 2, 4, 5)
    widths = [weights[w].shape[1] // inner for w in range(5)]
    offsets = [sum(widths[:w]) for w in range(5)]
    shard = weights[0].shape[0]
    result_rows = weights[5].shape[0] // inner
    down_rows = weights[8].shape[0] // members
    split = pieces_of(shard, 2)
    chunks = [(w, k * (shard // split), shard // split) for k in range(split) for w in (6, 7)]
    split = pieces_of(down_rows, 2)
    size = down_rows // split
    chunks += [(8, k * size, size) for k in range(split)]
    count = len(chunks)

    def kernel(*refs):
        sources = refs[:9]
        (features_ref, gain_ref, shift_ref, spike_ref, scale_ref) = refs[9:14]
        (second_ref, content_taps_ref, switch_taps_ref, out_ref) = refs[14:18]
        (project_all, result_all, expand_all, contract_all) = refs[18:22]
        (whole_ref, normed_ref, spike_all, gated_ref, stage, slot_a, held, slot_b) = refs[22:30]
        (mid_all, normed_mid, hidden_ref, down_stage, slot_d, own_part, held_down, slot_c) = refs[
            30:38
        ]
        (far_send, far_recv, near_send, near_recv, own_sem) = refs[38:43]
        (spike_send, spike_recv, mix_send, mix_recv, cross_send, cross_recv) = refs[43:49]
        (group_send, group_recv, y_send, y_recv, z_send, z_recv) = refs[49:55]
        second_spread = refs[55:61]
        (down_send, down_recv, back_send, back_recv, pass_send, held_twin) = refs[61:67]
        (x_send, x_recv, first_sem) = refs[67:70]
        rep, fs, tp = lax.axis_index("rep"), lax.axis_index("fs"), lax.axis_index("tp")
        a, b = fs // inner, lax.rem(fs, inner)
        p = lax.rem(a, n_pair)
        far = [partner(a, d, outer) for d in range(1, outer)]
        near = [a * inner + lax.rem(b + d, inner) for d in range(1, inner)]
        tps = [lax.rem(tp + d, n_tp) for d in range(1, n_tp)]
        reps = [lax.rem(rep + d, n_rep) for d in range(1, n_rep)]
        sides = [lax.rem(b + d, inner) for d in range(1, inner)]
        group = [
            {"fs": a * inner + lax.rem(b + i, inner), "tp": lax.rem(tp + j, n_tp)}
            for i in range(inner)
            for j in range(n_tp)
            if i or j
        ]
        team = []
        diagonal = []
        for i in range(n_rep):
            for j in range(n_pair):
                if i or j:
                    r, q = lax.rem(rep + i, n_rep), lax.rem(p + j, n_pair)
                    peer = {"rep": r, "fs": (a - p + q) * inner + b}
                    team.append((peer, r * n_pair + q))
                    if i and j:
                        diagonal.append(peer)
        me = rep * n_pair + p
        twin = rep * n_pair + lax.rem(p + 1, n_pair)
        twin_peer = {"fs": (a - p + lax.rem(p + 1, n_pair)) * inner + b}
        between = lax.rem(a + 1, outer) // 2 == 1
        greeted = [{"fs": index * inner + b} for index in far]
        greeted += group + diagonal + [{"rep": index} for index in reps]
        barrier = pltpu.get_barrier_semaphore()
        for peer in greeted:
            pl.semaphore_signal(barrier, inc=1, device_id=peer, device_id_type=MESH)
        pl.semaphore_wait(barrier, len(greeted))

        def at(start, size):
            return pl.ds(pl.multiple_of(start, size), size)

        def source(c, position):
            w, start, size = chunks[c]
            member = rep * n_pair + lax.rem(position, n_pair)
            if w < 8:
                return sources[w].at[pl.ds(start, size), at(member * units, units)]
            base = pl.multiple_of(member * down_rows, down_rows)
            return sources[w].at[pl.ds(base + start, size), :]

        def block(c, index):
            w, start, size = chunks[c]
            if w < 8:
                base = pl.multiple_of(index * shard, shard)
                return expand_all.at[pl.ds(base + start, size), pl.ds((w - 6) * units, units)]
            return contract_all.at[pl.ds(start, size), at(index * side, side)]

        def origin(k, lanes_of, planes=n_rep):
            w = firsts[k]
            size = (result_rows if w == 5 else shard) // planes
            start = rep * size if planes > 1 else 0
            if w == 5:
                return sources[w].at[at(lanes_of * result_rows + start, size), :]
            return sources[w].at[at(start, size), at(lanes_of * widths[w], widths[w])]

        def landing(k, index, planes=n_rep):
            w = firsts[k]
            size = (result_rows if w == 5 else shard) // planes
            start = rep * size if planes > 1 else 0
            if w == 5:
                return result_all.at[at(start, size), at(index * side, side)]
            return project_all.at[at(index * shard + start, size), pl.ds(offsets[w], widths[w])]

        sent, passed = [], []
        near_copies, own_copies = {}, {}

        def send_far(c, d, slot, position):
            copy = send_to(
                source(c, position),
                block(c, fs),
                far_send.at[c, d],
                far_recv.at[c, slot],
                {"fs": position * inner + b},
            )
            sent.append(copy)

        def launch_far(c, steps):
            for d in steps:
                send_far(c, d, d, far[d])

        def launch_middle(c):
            send_far(c, 1, jnp.where(between, 2, 1), jnp.where(between, far[2], far[1]))

        def launch_end(c):
            send_far(c, 2, jnp.where(between, 1, 2), jnp.where(between, far[1], far[2]))
            send_far(c, 0, 0, far[0])

        def landed_far(c, d):
            landed = block(c, far[d] * inner + b)
            pltpu.make_async_remote_copy(
                src_ref=landed,
                dst_ref=landed,
                send_sem=far_send.at[c, d],
                recv_sem=far_recv.at[c, d],
                device_id={"fs": far[d] * inner + b},
                device_id_type=MESH,
            ).wait_recv()
            return landed

        def launch_near(c):
            near_copies[c] = [
                send_to(
                    source(c, a),
                    block(c, fs),
                    near_send.at[c, 0, e],
                    near_recv.at[c, 0, e],
                    {"fs": index},
                )
                for e, index in enumerate(near)
            ]
            sent.extend(near_copies[c])
            own_copies[c] = pltpu.make_async_copy(source(c, a), block(c, fs), own_sem.at[c])
            own_copies[c].start()

        def forward(c):
            for d in range(outer - 1):
                landed = landed_far(c, d)
                copies = [
                    send_to(
                        landed,
                        landed,
                        near_send.at[c, d + 1, e],
                        near_recv.at[c, d + 1, e],
                        {"fs": index},
                    )
                    for e, index in enumerate(near)
                ]
                near_copies[c] += copies
                sent.extend(copies)

        def arrived(c):
            for copy in near_copies[c]:
                copy.wait_recv()
            own_copies[c].wait()

        third = [c for c in range(count) if chunks[c][0] < 8]
        fourth = [c for c in range(count) if chunks[c][0] == 8]
        relayed = outer == 4
        every = range(outer - 1)

        parts = [(h * (length // pieces), length // pieces) for h in range(pieces)]

        def spread(ref, sems):
            pair_send, pair_recv, across_send, across_recv, strip_send, strip_recv = sems
            pair_copies, across_copies, strip_copies = {}, {}, []

            def rows_of(member, h):
                start, size = parts[h]
                base = pl.multiple_of(member * length, length)
                return ref.at[pl.ds(base + start, size), at(tp * columns, columns)]

            def across(j, h):
                member = rep * n_pair + lax.rem(p + n_pair - j, n_pair)
                for i, index in enumerate(reps):
                    copy = send_to(
                        rows_of(member, h),
                        rows_of(member, h),
                        across_send.at[i, j, h],
                        across_recv.at[i, j, h],
                        {"rep": index},
                    )
                    across_copies[i, j, h] = copy
                    sent.append(copy)

            def strips(member):
                strip = ref.at[at(member * length, length), at(tp * columns, columns)]
                k = len(strip_copies)
                copies = [
                    send_to(strip, strip, strip_send.at[k, d], strip_recv.at[k, d], {"tp": index})
                    for d, index in enumerate(tps)
                ]
                strip_copies.append((member, copies))
                sent.extend(copies)

            def begin():
                for h in range(pieces):
                    for j in range(1, n_pair):
                        index = (a - p + lax.rem(p + j, n_pair)) * inner + b
                        copy = send_to(
                            rows_of(me, h),
                            rows_of(me, h),
                            pair_send.at[j - 1, h],
                            pair_recv.at[j - 1, h],
                            {"fs": index},
                        )
                        pair_copies[j, h] = copy
                        sent.append(copy)
                for h in range(pieces):
                    across(0, h)
                strips(me)

            def relay(h):
                for j in range(1, n_pair):
                    pair_copies[j, h].wait_recv()
                    across(j, h)
                    if h == pieces - 1:
                        strips(rep * n_pair + lax.rem(p + n_pair - j, n_pair))

            def complete(j):
                for i in range(1, n_rep):
                    for h in range(pieces):
                        across_copies[i - 1, j, h].wait_recv()
                    r = lax.rem(rep + n_rep - i, n_rep)
                    strips(r * n_pair + lax.rem(p + n_pair - j, n_pair))

            return begin, relay, complete, strip_copies

        y_copies, x_copies, first_copies = {}, {}, []

        def shard_of(e, d):
            position = a if d == 0 else far[d - 1]
            return position * inner + lax.rem(b + inner - e, inner)

        def aside(k):
            for e, index in enumerate(sides):
                y_copies[k, e + 1] = send_to(
                    origin(k, index),
                    landing(k, fs),
                    y_send.at[k, e],
                    y_recv.at[k, e],
                    {"fs": a * inner + index},
                )
                sent.append(y_copies[k, e + 1])
            copy = pltpu.make_async_copy(
                origin(k, b, 1), landing(k, fs, 1), first_sem.at[k]
            )
            copy.start()
            first_copies.append(copy)

        def along(k, e):
            index = shard_of(e, 0)
            start = landing(k, index) if e else origin(k, b)
            if relayed:
                middle = (jnp.where(between, 2, 1), jnp.where(between, far[2], far[1]))
                steps = [(0, 0, far[0]), (1,) + middle]
            else:
                steps = [(d, d, far[d]) for d in every]
            for d, slot, position in steps:
                copy = send_to(
                    start,
                    landing(k, index),
                    z_send.at[k, e, d],
                    z_recv.at[k, e, slot],
                    {"fs": position * inner + b},
                )
                sent.append(copy)

        def line_copy(k, e, d, send_sem, slot):
            landed = landing(k, shard_of(e, d + 1))
            return pltpu.make_async_remote_copy(
                src_ref=landed,
                dst_ref=landed,
                send_sem=send_sem,
                recv_sem=z_recv.at[k, e, slot],
                device_id={"fs": far[0] * inner + b},
                device_id_type=MESH,
            )

        def passed_on(k, e, d):
            return line_copy(k, e, d, pass_send.at[k, e, d], 3 - d)

        def cross_plane(k, e, d):
            landed = landing(k, shard_of(e, d))
            for i, index in enumerate(reps):
                x_copies[k, e, d, i] = send_to(
                    landed,
                    landed,
                    x_send.at[k, e, d, i],
                    x_recv.at[k, e, d, i],
                    {"rep": index},
                )
                sent.append(x_copies[k, e, d, i])

        def carry_on(k):
            for d in every:
                for e in range(inner):
                    line_copy(k, e, d, z_send.at[k, e, d], d).wait_recv()
                    if relayed and d > 0:
                        passed.append((k, e, d))

                        @pl.when(between)
                        def _():
                            passed_on(k, e, d).start()

                    cross_plane(k, e, d + 1)

        def settled(k):
            first_copies[k].wait()
            for (at_k, e, d, i), copy in x_copies.items():
                if at_k == k:
                    copy.wait_recv()

        for k in range(len(firsts)):
            aside(k)
            along(k, 0)
        spot = whole_ref.at[at(b * length, length), at(tp * columns, columns)]
        own_features = pltpu.make_async_copy(features_ref, spot, own_sem.at[count])
        own_features.start()
        group_copies = [
            send_to(features_ref, spot, group_send.at[d], group_recv.at[d], peer)
            for d, peer in enumerate(group)
        ]
        lines = spike_all.at[at(b * length, length), :]
        own_spike = pltpu.make_async_copy(
            spike_ref.at[:, at(b * key_lanes, key_lanes)], lines, own_sem.at[count + 1]
        )
        own_spike.start()
        group_copies += [
            send_to(
                spike_ref.at[:, at(index * key_lanes, key_lanes)],
                lines,
                spike_send.at[d],
                spike_recv.at[d],
                {"fs": a * inner + index},
            )
            for d, index in enumerate(sides)
        ]
        for k in range(len(firsts)):
            for e in range(1, inner):
                y_copies[k, e].wait_recv()
                along(k, e)
                cross_plane(k, e, 0)
        for c in third:
            if relayed:
                launch_middle(c)
            else:
                launch_far(c, every)
        for c in third + fourth:
            launch_near(c)
        for k in range(len(firsts)):
            carry_on(k)
        if relayed:
            for c in third:
                launch_end(c)
            for c in fourth:
                launch_middle(c)
        own_features.wait()
        own_spike.wait()
        for copy in group_copies:
            copy.wait()

        def first_norm(i, carry):
            lines = at(i * length, length)
            normed_ref[lines, :] = row_norm(whole_ref[lines, :], gain_ref[...])
            return carry

        lax.fori_loop(0, inner, first_norm, 0)
        for k in range(len(firsts)):
            if firsts[k] != 5:
                settled(k)

        def attention(index):
            lines = at(index * length, length)
            sums = jnp.dot(normed_ref[lines, :], project_all[...], preferred_element_type=F32)
            gated_ref[lines, :] = attend_rows(
                sums,
                shift_ref[:, at(b * key_lanes, key_lanes)],
                spike_all[lines, :],
                scale_ref[:, at(b * value_lanes, value_lanes)].astype(F32),
                heads,
            )

        half = len(third) // 2
        order = sides + [b]
        for index in order:
            attention(index)
        settled(firsts.index(5))

        def mixed(index, strip):
            return jnp.dot(
                gated_ref[at(index * length, length), :],
                result_all[:, at(strip * columns, columns)],
                preferred_element_type=F32,
            )

        mix_copies = []
        for i, index in enumerate(order):
            copies = []
            for d, other in enumerate(tps):
                stage[i, d] = mixed(index, other).astype(BF16)
                copies.append(
                    send_to(
                        stage.at[i, d],
                        slot_a.at[i, d],
                        mix_send.at[i, d],
                        mix_recv.at[i, d],
                        {"tp": other},
                    )
                )
            mix_copies.append(copies)
            sent.extend(copies)
        cross_copies = []
        for i, index in enumerate(order):
            total = mixed(index, tp)
            for d, copy in enumerate(mix_copies[i]):
                copy.wait_recv()
                total = total + slot_a[i, d].astype(F32)
            if i < inner - 1:
                held[i] = total.astype(BF16)
                copy = send_to(
                    held.at[i],
                    slot_b.at[i],
                    cross_send.at[i],
                    cross_recv.at[i],
                    {"fs": a * inner + index},
                )
                cross_copies.append(copy)
                sent.append(copy)
            else:
                for d, copy in enumerate(cross_copies):
                    copy.wait_recv()
                    total = total + slot_b[d].astype(F32)
        base = whole_ref[at(b * length, length), at(tp * columns, columns)].astype(F32)
        mine = mid_all.at[at(me * length, length), at(tp * columns, columns)]
        mine[...] = (base + total.astype(BF16).astype(F32)).astype(BF16)

        begin, relay, complete, blocks = spread(mid_all, second_spread)
        begin()
        for c in fourth:
            if relayed:
                launch_end(c)
            else:
                launch_far(c, every)
        for c in third:
            forward(c)
        for h in range(pieces):
            relay(h)
        for j in range(n_pair):
            complete(j)

        def second_norm(member):
            lines = at(member * length, length)
            normed_mid[lines, :] = row_norm(mid_all[lines, :], second_ref[...])

        for member, copies in blocks:
            for copy in copies:
                copy.wait_recv()
            second_norm(member)
        for c in fourth:
            forward(c)
        for c in third:
            arrived(c)

        def expand(i, carry):
            lines = at(i * length, length)
            both = jnp.dot(normed_mid[lines, :], expand_all[...], preferred_element_type=F32)
            both = both.astype(BF16).astype(F32)
            value = taps_sum(both[:, :units], content_taps_ref[:, at(me * units, units)])
            gate = taps_sum(both[:, units:], switch_taps_ref[:, at(me * units, units)])
            hidden_ref[lines, :] = (value * jax.nn.gelu(gate, approximate=True)).astype(BF16)
            return carry

        lax.fori_loop(0, members, expand, 0)

        crossing = [
            (i, j, index * n_pair + lax.rem(p + j, n_pair))
            for j in reversed(range(n_pair))
            for i, index in enumerate(reps)
        ]
        turn = len(crossing)

        back_copies = {}
        pending, turning = [], []

        def finish(e, run, lanes, copies):
            total = own_part[:, lanes]
            for d, copy in enumerate(copies):
                copy.wait_recv()
                total = total + slot_d[d, :, lanes].astype(F32)
            own_part[:, lanes] = total
            held_down[:, lanes] = total.astype(BF16)
            for k, (i, j, member) in enumerate(crossing):
                back_copies[e, run, k] = send_to(
                    held_down.at[at(member * length, length), lanes],
                    slot_c.at[k, :, lanes],
                    back_send.at[e, run, k],
                    back_recv.at[e, run, k],
                    {"rep": reps[i]},
                )

        def turned(e, run, lanes):
            total = own_part[at(twin * length, length), lanes]
            for k, (i, j, member) in enumerate(crossing):
                if j:
                    back_copies[e, run, k].wait_recv()
                    total = total + slot_c[k, :, lanes].astype(F32)
            held_twin[:, lanes] = total.astype(BF16)
            back_copies[e, run, turn] = send_to(
                held_twin.at[:, lanes],
                slot_c.at[turn, :, lanes],
                back_send.at[e, run, turn],
                back_recv.at[e, run, turn],
                twin_peer,
            )

        for e in range(inner):
            lane = lax.rem(b + inner - e, inner)
            waited = set()

            def weights_of(run):
                for c in fourth:
                    for d in range(run, outer, runs) if aligned else range(outer):
                        if (c, d) in waited:
                            continue
                        waited.add((c, d))
                        if e:
                            near_copies[c][d * (inner - 1) + e - 1].wait_recv()
                        elif d == 0:
                            own_copies[c].wait()

            def spot(run):
                place = lax.rem(p + run, runs) if aligned else run
                return place, at((place * inner + lane) * side, side)

            def product(strip, place):
                index = (strip * runs + place) * inner + lane
                return jnp.dot(
                    hidden_ref[...],
                    contract_all[:, at(index * side, side)],
                    preferred_element_type=F32,
                )

            for run in range(runs):
                weights_of(run)
                place, lanes = spot(run)
                copies = []
                for d, other in enumerate(tps):
                    down_stage[d, :, lanes] = product(other, place).astype(BF16)
                    copies.append(
                        send_to(
                            down_stage.at[d, :, lanes],
                            slot_d.at[d, :, lanes],
                            down_send.at[e, run, d],
                            down_recv.at[e, run, d],
                            {"tp": other},
                        )
                    )
                sent.extend(copies)
                own_part[:, lanes] = product(tp, place)
                for step in turning:
                    turned(*step[:3])
                turning = pending
                for step in pending:
                    finish(*step)
                pending = [(e, run, lanes, copies)]
        for step in pending:
            finish(*step)
        for step in turning + pending:
            turned(*step[:3])
        for (e, run, k), copy in back_copies.items():
            if k == turn or not crossing[k][1]:
                copy.wait_recv()
        total = own_part[at(me * length, length), :]
        for k in [turn] + [k for k in range(turn) if not crossing[k][1]]:
            total = total + slot_c[k].astype(F32)
        out_ref[...] = (mine[...].astype(F32) + total.astype(BF16).astype(F32)).astype(BF16)
        for copy in sent + list(back_copies.values()):
            copy.wait_send()
        if passed:

            @pl.when(between)
            def _():
                for step in passed:
                    passed_on(*step).wait_send()

    dma = pltpu.SemaphoreType.DMA
    vmem = pl.BlockSpec(memory_space=pltpu.VMEM)
    hbm = pl.BlockSpec(memory_space=pl.ANY)

    def pair(*shape):
        shape = tuple(max(n, 1) for n in shape)
        return [dma(shape), dma(shape)]

    def room(*shape, dtype=BF16):
        return pltpu.VMEM(tuple(max(n, 1) for n in shape), dtype)

    scratch = [
        room(shard * n_fs, sum(widths)),
        room(result_rows, side * n_fs),
        room(shard * n_fs, 2 * units),
        room(down_rows, side * n_fs),
        room(rows, wide),
        room(rows, wide),
        room(rows, key_lanes, dtype=F32),
        room(rows, value_lanes),
        room(inner, n_tp - 1, length, columns),
        room(inner, n_tp - 1, length, columns),
        room(inner - 1, length, columns),
        room(inner - 1, length, columns),
        room(tokens, wide),
        room(tokens, wide),
        room(tokens, units),
        room(n_tp - 1, tokens, columns),
        room(n_tp - 1, tokens, columns),
        room(tokens, columns, dtype=F32),
        room(tokens, columns),
        room(members - 1, length, columns),
    ]
    scratch += pair(count, outer - 1) + pair(count, outer, inner - 1) + [dma((count + 2,))]
    many = len(firsts)
    scratch += pair(inner - 1) + pair(inner, n_tp - 1) + pair(inner - 1)
    scratch += pair(inner * n_tp - 1) + pair(many, inner - 1) + pair(many, inner, outer - 1)
    scratch += pair(n_pair - 1, pieces) + pair(n_rep - 1, n_pair, pieces)
    scratch += pair(members, n_tp - 1)
    scratch += pair(inner, runs, n_tp - 1) + pair(inner, runs, members - 1)
    scratch += [dma((many, inner, max(outer - 1, 1))), room(length, columns)]
    scratch += pair(many, inner, outer, n_rep - 1) + [dma((many,))]
    return pl.pallas_call(
        kernel,
        out_shape=jax.ShapeDtypeStruct((length, columns), BF16),
        in_specs=[hbm] * 10 + [vmem] * 7,
        out_specs=vmem,
        scratch_shapes=scratch,
        compiler_params=pltpu.CompilerParams(
            collective_id=0, has_side_effects=True, vmem_limit_bytes=VMEM_LIMIT
        ),
        name="whole_layer",
    )(
        *weights,
        features,
        first_gain.reshape(1, -1),
        shift.reshape(1, -1),
        spike,
        scale.reshape(1, -1),
        second_gain.reshape(1, -1),
        content_taps,
        switch_taps,
    )


def shards(
    sizes,
    incoming_features,
    attend_prenormal_scale,
    probe_matrix,
    lookup_matrix,
    content_matrix,
    forgetting_matrix,
    result_switch_matrix,
    forgetting_shift,
    spike_forget_logarithm,
    attend_unit_scale,
    attend_result_matrix,
    perceptron_scale,
    content_expand_matrix,
    switch_expand_matrix,
    content_kernel,
    switch_kernel,
    contract_matrix,
):
    n_rep, n_fs, n_tp = sizes
    rep = lax.axis_index("rep")
    length = incoming_features.shape[0]
    if fits(
        sizes, incoming_features, probe_matrix, attend_result_matrix, content_expand_matrix
    ):
        return whole_layer(
            sizes,
            incoming_features,
            attend_prenormal_scale,
            (
                probe_matrix,
                lookup_matrix,
                content_matrix,
                forgetting_matrix,
                result_switch_matrix,
                attend_result_matrix,
                content_expand_matrix,
                switch_expand_matrix,
                contract_matrix,
            ),
            forgetting_shift,
            spike_forget_logarithm,
            attend_unit_scale,
            perceptron_scale,
            content_kernel,
            switch_kernel,
        )

    def mine(array, axis):
        size = array.shape[axis] // n_rep
        return lax.dynamic_slice_in_dim(array, rep * size, size, axis)

    project = jnp.concatenate(
        [
            mine(matrix, 1)
            for matrix in (
                probe_matrix,
                lookup_matrix,
                content_matrix,
                forgetting_matrix,
                result_switch_matrix,
            )
        ],
        axis=1,
    )
    spike_all = lax.all_to_all(
        spike_forget_logarithm, "rep", split_axis=1, concat_axis=0, tiled=True
    )
    expand = jnp.concatenate([mine(content_expand_matrix, 1), mine(switch_expand_matrix, 1)], axis=1)
    side = attend_result_matrix.shape[1]
    inside = side % 128 == 0
    outs = first_half(
        project,
        mine(attend_result_matrix, 0),
        expand,
        mine(contract_matrix, 0),
        incoming_features,
        attend_prenormal_scale,
        mine(forgetting_shift, 0),
        spike_all,
        mine(attend_unit_scale, 0),
        1 if inside else 0,
        inside,
        sizes,
    )
    if inside:
        expand_all, contract_all, middle, whole_mid = outs
    else:
        expand_all, contract_all, result_all, switched_result = outs
        result_all, contract_all = (
            array.reshape(n_fs, -1, side).swapaxes(0, 1).reshape(-1, n_fs * side)
            for array in (result_all, contract_all)
        )
        mixer_partial = jnp.dot(switched_result, result_all, preferred_element_type=F32)
        middle, whole_mid = reduce_group(
            mixer_partial.astype(BF16), incoming_features, sizes, True, 2
        )
    normed_mid = row_norm(whole_mid, perceptron_scale)
    both = jnp.dot(normed_mid, expand_all, preferred_element_type=F32).astype(BF16)
    half = both.shape[1] // 2
    conv_value = causal_conv(both[:, :half], mine(content_kernel, 1), length)
    conv_gated = causal_conv(both[:, half:], mine(switch_kernel, 1), length)
    hidden = (conv_value * jax.nn.gelu(conv_gated, approximate=True)).astype(BF16)
    down_partial = jnp.dot(hidden, contract_all, preferred_element_type=F32).astype(BF16)
    return reduce_group(down_partial, middle, sizes, False, 3)[0]


def solution(mesh):
    sizes = (mesh.shape["rep"], mesh.shape["fs"], mesh.shape["tp"])
    placed = (
        P(("rep", "fs"), "tp"),
        P(),
        P("fs", "tp"),
        P("fs", "tp"),
        P("fs", "tp"),
        P("fs", "tp"),
        P("fs", "tp"),
        P("tp"),
        P(("rep", "fs"), "tp"),
        P("tp"),
        P("tp", "fs"),
        P(),
        P("fs", "tp"),
        P("fs", "tp"),
        P(None, "tp"),
        P(None, "tp"),
        P("tp", "fs"),
    )
    return jax.shard_map(
        functools.partial(shards, sizes),
        mesh=mesh,
        in_specs=placed,
        out_specs=P(("rep", "fs"), "tp"),
        check_vma=False,
    )
```

```python
import functools

import jax
import jax.numpy as jnp
from jax import lax
from jax.experimental import pallas as pl
from jax.experimental.pallas import tpu as pltpu
from jax.sharding import PartitionSpec as P

HEAD_K = 32
HEAD_V = 64
SUB = 16

norm_eps = 1e-06
switch_multiplier = 16.0
MESH = pl.DeviceIdType.MESH
F32 = jnp.float32
BF16 = jnp.bfloat16
VMEM_LIMIT = 60 * 1024 * 1024


def row_norm(content_tokens, gain):
    content_tokens = content_tokens.astype(F32)
    scaled = content_tokens * lax.rsqrt(
        jnp.mean(content_tokens * content_tokens, axis=-1, keepdims=True) + norm_eps
    )
    return (scaled * gain.astype(F32)).astype(BF16)


def factor(n):
    inner = 1
    for size in range(1, n + 1):
        if n % size == 0 and size * size <= n:
            inner = size
    return n // inner, inner


def place(ref, axis, index, size):
    at = pl.ds(pl.multiple_of(index * size, size), size)
    return ref.at[at, :] if axis == 0 else ref.at[:, at]


def send_to(source, target, send_sem, recv_sem, peer):
    copy = pltpu.make_async_remote_copy(
        src_ref=source,
        dst_ref=target,
        send_sem=send_sem,
        recv_sem=recv_sem,
        device_id=peer,
        device_id_type=MESH,
    )
    copy.start()
    return copy


def pieces_of(rows, most):
    for count in range(most, 1, -1):
        if rows % (16 * count) == 0:
            return count
    return 1


def first_half(
    project, result, expand, contract, features, gain, shift, spike, scale, axis, inside, sizes
):
    n_rep, n_fs, n_tp = sizes
    outer, inner = factor(n_fs)
    length, columns = features.shape
    rows = length * n_rep
    heads = shift.shape[0] // HEAD_K
    value_lanes = heads * HEAD_V
    group = n_rep * n_tp
    most = max(n_rep, n_tp)
    weights = (project, result, expand, contract)
    axes = (0, axis, 0, axis)
    splits = (2, 1, 4, 4)
    full = []
    chunks = []
    for w in range(4):
        shape = list(weights[w].shape)
        size = shape[0]
        shape[axes[w]] *= n_fs
        full.append(tuple(shape))
        split = pieces_of(size, splits[w])
        chunks += [(w, k * (size // split), size // split) for k in range(split)]
    count = len(chunks)

    def kernel(*refs):
        sources = refs[:4]
        features_ref, gain_ref, shift_ref, spike_ref, scale_ref = refs[4:9]
        if inside:
            expand_out, contract_out, middle_ref, mid_ref = refs[9:13]
            rest = refs[13:]
            result_out, gated_ref, partial_ref, slot_a, held, slot_b = rest[:6]
            rest = rest[6:]
        else:
            expand_out, contract_out, result_out, gated_ref = refs[9:13]
            rest = refs[13:]
        project_out, whole_ref = rest[:2]
        far_send, far_recv, near_send, near_recv, own_sem, group_send, group_recv = rest[2:9]
        if inside:
            sum_send, sum_recv = rest[9:]
        outs = (project_out, result_out, expand_out, contract_out)
        rep, fs, tp = lax.axis_index("rep"), lax.axis_index("fs"), lax.axis_index("tp")
        a, b = fs // inner, lax.rem(fs, inner)
        far = [lax.rem(a + d, outer) * inner + b for d in range(1, outer)]
        near = [a * inner + lax.rem(b + d, inner) for d in range(1, inner)]
        peers = [{"fs": index} for index in far + near]
        others = [
            {"rep": lax.rem(rep + i, n_rep), "tp": lax.rem(tp + j, n_tp)}
            for i in range(n_rep)
            for j in range(n_tp)
            if i or j
        ]
        barrier = pltpu.get_barrier_semaphore()
        for peer in peers + others:
            pl.semaphore_signal(barrier, inc=1, device_id=peer, device_id_type=MESH)
        pl.semaphore_wait(barrier, len(peers) + len(others))

        def block(w, start, size, index):
            across = weights[w].shape[axes[w]]
            offset = pl.multiple_of(index * across, across)
            if axes[w] == 0:
                return outs[w].at[pl.ds(offset + start, size), :]
            return outs[w].at[pl.ds(start, size), pl.ds(offset, across)]

        far_copies, near_copies, own_copies = {}, {}, {}

        def launch_far(c):
            w, start, size = chunks[c]
            source, target = sources[w].at[pl.ds(start, size), :], block(w, start, size, fs)
            far_copies[c] = [
                send_to(source, target, far_send.at[c, d], far_recv.at[c, d], {"fs": index})
                for d, index in enumerate(far)
            ]

        def launch_near(c):
            w, start, size = chunks[c]
            source, target = sources[w].at[pl.ds(start, size), :], block(w, start, size, fs)
            near_copies[c] = [
                send_to(
                    source, target, near_send.at[c, 0, e], near_recv.at[c, 0, e], {"fs": index}
                )
                for e, index in enumerate(near)
            ]
            own_copies[c] = pltpu.make_async_copy(source, target, own_sem.at[c])
            own_copies[c].start()

        def forward(c):
            w, start, size = chunks[c]
            for d in range(1, outer):
                far_copies[c][d - 1].wait_recv()
                held_block = block(w, start, size, lax.rem(a + outer - d, outer) * inner + b)
                near_copies[c] += [
                    send_to(
                        held_block,
                        held_block,
                        near_send.at[c, d, e],
                        near_recv.at[c, d, e],
                        {"fs": index},
                    )
                    for e, index in enumerate(near)
                ]

        def arrived(c):
            for copy in near_copies[c]:
                copy.wait_recv()
            own_copies[c].wait()

        first = [c for c in range(count) if chunks[c][0] == 0]
        second = [c for c in range(count) if chunks[c][0] == 1]
        later = [c for c in range(count) if chunks[c][0] > 1]

        spot = whole_ref.at[
            pl.ds(pl.multiple_of(rep * length, length), length),
            pl.ds(pl.multiple_of(tp * columns, columns), columns),
        ]
        own = pltpu.make_async_copy(features_ref, spot, own_sem.at[count])
        own.start()
        group_copies = [
            send_to(features_ref, spot, group_send.at[d], group_recv.at[d], peer)
            for d, peer in enumerate(others)
        ]
        for c in first:
            launch_far(c)
            launch_near(c)
        for c in second + later:
            launch_far(c)
        for c in first:
            forward(c)
        for c in second + later:
            launch_near(c)
        for c in first:
            arrived(c)
        own.wait()
        for copy in group_copies:
            copy.wait()

        def sequence(i, carry):
            at = pl.ds(pl.multiple_of(i * length, length), length)
            normed = row_norm(whole_ref[at, :], gain_ref[...])
            sums = jnp.dot(normed, project_out[...], preferred_element_type=F32)
            gated_ref[at, :] = attend_rows(
                sums, shift_ref[...], spike_ref[at, :], scale_ref[...], heads
            )
            return carry

        lax.fori_loop(0, n_rep, sequence, 0)
        for c in second:
            forward(c)
        waiting = list(later)
        for c in waiting[:1]:
            forward(c)
        waiting = waiting[1:]
        for c in second:
            arrived(c)
        if inside:

            def mixer(i, carry):
                at = pl.ds(pl.multiple_of(i * length, length), length)
                partial_ref[at, :] = jnp.dot(
                    gated_ref[at, :], result_out[...], preferred_element_type=F32
                ).astype(BF16)
                return carry

            lax.fori_loop(0, n_rep, mixer, 0)

            def between(stage):
                if stage in (1, 2):
                    forward(waiting.pop(0))

            reduce_steps(
                partial_ref,
                features_ref,
                middle_ref,
                mid_ref,
                slot_a,
                held,
                slot_b,
                sum_send,
                sum_recv,
                sizes,
                between,
            )
        for c in waiting:
            forward(c)
        for c in later:
            arrived(c)
        for c in range(count):
            for copy in far_copies[c] + near_copies[c]:
                copy.wait_send()

    dma = pltpu.SemaphoreType.DMA
    vmem = pl.BlockSpec(memory_space=pltpu.VMEM)
    hbm = pl.BlockSpec(memory_space=pl.ANY)
    out_shape = [jax.ShapeDtypeStruct(full[2], BF16), jax.ShapeDtypeStruct(full[3], BF16)]
    scratch = []
    gated_shape = (rows, value_lanes)
    if inside:
        out_shape += [
            jax.ShapeDtypeStruct((length, columns), BF16),
            jax.ShapeDtypeStruct((rows, columns * n_tp), BF16),
        ]
        out_specs = [hbm, hbm, vmem, vmem]
        scratch += [
            pltpu.VMEM(full[1], BF16),
            pltpu.VMEM(gated_shape, BF16),
            pltpu.VMEM((rows, columns * n_tp), BF16),
            pltpu.VMEM((max(n_tp - 1, 1), rows, columns), BF16),
            pltpu.VMEM((rows, columns), BF16),
            pltpu.VMEM((max(n_rep - 1, 1), length, columns), BF16),
        ]
    else:
        out_shape += [
            jax.ShapeDtypeStruct(full[1], BF16),
            jax.ShapeDtypeStruct(gated_shape, BF16),
        ]
        out_specs = [hbm, hbm, hbm, vmem]
    scratch += [
        pltpu.VMEM(full[0], BF16),
        pltpu.VMEM((rows, columns * n_tp), BF16),
        dma((count, max(outer - 1, 1))),
        dma((count, max(outer - 1, 1))),
        dma((count, outer, max(inner - 1, 1))),
        dma((count, outer, max(inner - 1, 1))),
        dma((count + 1,)),
        dma((group,)),
        dma((group,)),
    ]
    if inside:
        scratch += [dma((4, most)), dma((4, most))]
    return pl.pallas_call(
        kernel,
        out_shape=out_shape,
        in_specs=[vmem] * 9,
        out_specs=out_specs,
        scratch_shapes=scratch,
        compiler_params=pltpu.CompilerParams(
            collective_id=0, has_side_effects=True, vmem_limit_bytes=VMEM_LIMIT
        ),
        name="first_half",
    )(
        *weights,
        features,
        gain.reshape(1, -1),
        shift.reshape(1, -1),
        spike,
        scale.astype(F32).reshape(1, -1),
    )


def reduce_steps(
    part_ref, base_ref, out_ref, all_ref, slot_a, held, slot_b, send_sem, recv_sem, sizes, between
):
    n_rep, n_fs, n_tp = sizes
    rows, columns = base_ref.shape
    rep, tp = lax.axis_index("rep"), lax.axis_index("tp")
    tps = [lax.rem(tp + d, n_tp) for d in range(1, n_tp)]
    reps = [lax.rem(rep + d, n_rep) for d in range(1, n_rep)]

    def send(stage, d, source, target, peer):
        return send_to(source, target, send_sem.at[stage, d], recv_sem.at[stage, d], peer)

    copies = [
        send(0, d, place(part_ref, 1, index, columns), slot_a.at[d], {"tp": index})
        for d, index in enumerate(tps)
    ]
    for copy in copies:
        copy.wait()
    total = place(part_ref, 1, tp, columns)[...].astype(F32)
    for d in range(len(tps)):
        total = total + slot_a[d].astype(F32)
    held[...] = total.astype(BF16)
    copies = [
        send(1, d, place(held, 0, index, rows), slot_b.at[d], {"rep": index})
        for d, index in enumerate(reps)
    ]
    between(1)
    for copy in copies:
        copy.wait()
    total = place(held, 0, rep, rows)[...].astype(F32)
    for d in range(len(reps)):
        total = total + slot_b[d].astype(F32)
    result = (base_ref[...].astype(F32) + total.astype(BF16).astype(F32)).astype(BF16)
    out_ref[...] = result
    if all_ref is not None:
        block = all_ref.at[
            pl.ds(pl.multiple_of(rep * rows, rows), rows),
            pl.ds(pl.multiple_of(tp * columns, columns), columns),
        ]
        block[...] = result
        copies = [send(2, d, block, block, {"rep": index}) for d, index in enumerate(reps)]
        between(2)
        for copy in copies:
            copy.wait()
        strip = place(all_ref, 1, tp, columns)
        copies = [send(3, d, strip, strip, {"tp": index}) for d, index in enumerate(tps)]
        for copy in copies:
            copy.wait()


def reduce_group(partial, base, sizes, spread, collective_id):
    n_rep, n_fs, n_tp = sizes
    rows, columns = base.shape

    def kernel(*refs):
        part_ref, base_ref = refs[:2]
        if spread:
            out_ref, all_ref, slot_a, held, slot_b, send_sem, recv_sem = refs[2:]
        else:
            all_ref = None
            out_ref, slot_a, held, slot_b, send_sem, recv_sem = refs[2:]
        rep, tp = lax.axis_index("rep"), lax.axis_index("tp")
        barrier = pltpu.get_barrier_semaphore()
        for d in range(1, n_tp):
            peer = {"tp": lax.rem(tp + d, n_tp)}
            pl.semaphore_signal(barrier, inc=1, device_id=peer, device_id_type=MESH)
        for d in range(1, n_rep):
            peer = {"rep": lax.rem(rep + d, n_rep)}
            pl.semaphore_signal(barrier, inc=1, device_id=peer, device_id_type=MESH)
        pl.semaphore_wait(barrier, n_tp + n_rep - 2)
        reduce_steps(
            part_ref,
            base_ref,
            out_ref,
            all_ref,
            slot_a,
            held,
            slot_b,
            send_sem,
            recv_sem,
            sizes,
            lambda stage: None,
        )

    out_shape = [jax.ShapeDtypeStruct((rows, columns), BF16)]
    if spread:
        out_shape.append(jax.ShapeDtypeStruct((rows * n_rep, columns * n_tp), BF16))
    vmem = pl.BlockSpec(memory_space=pltpu.VMEM)
    most = max(n_rep, n_tp)
    return pl.pallas_call(
        kernel,
        out_shape=out_shape,
        in_specs=[vmem, vmem],
        out_specs=[vmem] * len(out_shape),
        scratch_shapes=[
            pltpu.VMEM((max(n_tp - 1, 1), rows * n_rep, columns), BF16),
            pltpu.VMEM((rows * n_rep, columns), BF16),
            pltpu.VMEM((max(n_rep - 1, 1), rows, columns), BF16),
            pltpu.SemaphoreType.DMA((4, most)),
            pltpu.SemaphoreType.DMA((4, most)),
        ],
        compiler_params=pltpu.CompilerParams(
            collective_id=collective_id, has_side_effects=True, vmem_limit_bytes=VMEM_LIMIT
        ),
        name="reduce_group",
    )(partial, base)


def lanes_same(shape, row_width, column_width):
    return (
        lax.broadcasted_iota(jnp.int32, shape, 0) // row_width
        == lax.broadcasted_iota(jnp.int32, shape, 1) // column_width
    ).astype(F32)


def dot32(left, right, contract=((1,), (0,))):
    return lax.dot_general(
        left.astype(BF16), right.astype(BF16), (contract, ((), ())), preferred_element_type=F32
    )


def attend_rows(sums, shift, spike, scale, heads):
    length = sums.shape[0]
    key_lanes, value_lanes = heads * HEAD_K, heads * HEAD_V

    def part(start, width):
        return sums[:, start : start + width]

    def rounded(array):
        return array.astype(BF16).astype(F32)

    query = rounded(part(0, key_lanes)) * HEAD_K ** (-0.5)
    keys = rounded(part(key_lanes, key_lanes))
    values = rounded(part(2 * key_lanes, value_lanes))
    decay_pre = part(2 * key_lanes + value_lanes, key_lanes) + shift
    gate = rounded(part(3 * key_lanes + value_lanes, value_lanes))
    log_sigmoid = jnp.minimum(decay_pre, 0.0) - jnp.log1p(jnp.exp(-jnp.abs(decay_pre)))
    c = log_sigmoid / switch_multiplier + spike
    row = lax.broadcasted_iota(jnp.int32, (length, key_lanes), 0)
    step = 1
    while step < length:
        c = c + jnp.where(row >= step, pltpu.roll(c, step, 0), 0.0)
        step *= 2

    spread = lanes_same((key_lanes, value_lanes), HEAD_K, HEAD_V)
    in_sub = lax.rem(row, SUB)
    out = dot32(query * keys, spread) * values
    for d in range(1, SUB):
        ok = in_sub >= d
        weight = jnp.exp(jnp.where(ok, c - pltpu.roll(c, d, 0), 0.0))
        product = jnp.where(ok, query * pltpu.roll(keys, d, 0) * weight, 0.0)
        out = out + dot32(product, spread) * pltpu.roll(values, d, 0)

    pieces = [jnp.zeros((SUB, value_lanes), F32)]
    stack = heads * SUB
    key_mask = lanes_same((stack, key_lanes), SUB, HEAD_K)
    value_mask = lanes_same((stack, value_lanes), SUB, HEAD_V)
    for start in range(SUB, length, SUB):
        edge = c[start - 1 : start]
        q_part = query[start : start + SUB] * jnp.exp(c[start : start + SUB] - edge)
        k_part = keys[:start] * jnp.exp(edge - c[:start])
        stacked = jnp.concatenate([q_part] * heads, axis=0) * key_mask
        scores = dot32(stacked, k_part, ((1,), (1,)))
        read = dot32(scores, values[:start]) * value_mask
        total = read[:SUB]
        for h in range(1, heads):
            total = total + read[h * SUB : (h + 1) * SUB]
        pieces.append(total)
    out = out + jnp.concatenate(pieces, axis=0)

    same = lanes_same((value_lanes, value_lanes), HEAD_V, HEAD_V)
    mean = dot32(out * out, same) / HEAD_V
    out = out * lax.rsqrt(mean + norm_eps) * scale
    return (out * (gate / (1.0 + jnp.exp(-gate)))).astype(BF16)


def causal_conv(content_tokens, taps, length):
    rows, columns = content_tokens.shape
    content_tokens = content_tokens.astype(F32).reshape(rows // length, length, columns)
    taps = taps.astype(F32)
    width = taps.shape[0]
    padded = jnp.pad(content_tokens, ((0, 0), (width - 1, 0), (0, 0)))
    total = jnp.zeros_like(content_tokens)
    for offset in range(width):
        total = total + padded[:, offset : offset + length] * taps[offset]
    return total.reshape(rows, columns)


def pair_size(outer):
    return 2 if outer % 2 == 0 else 1


def fits(sizes, features, probe, result, content):
    n_rep, n_fs, n_tp = sizes
    outer, inner = factor(n_fs)
    members = n_rep * pair_size(outer)
    return (
        features.shape[0] % 16 == 0
        and features.shape[1] % 128 == 0
        and probe.shape[0] % (16 * n_rep) == 0
        and probe.shape[1] % (128 * inner) == 0
        and result.shape[1] % 128 == 0
        and result.shape[0] % (128 * inner * n_rep) == 0
        and content.shape[1] % (128 * members) == 0
        and outer & (outer - 1) == 0
        and members == 2 * n_rep
        and outer % n_tp == 0
    )


def partner(a, d, outer):
    total, bit = 0, 1
    while bit < outer:
        total = total + lax.rem(a // bit + (d // bit) % 2, 2) * bit
        bit *= 2
    return total


def shifted(array, step, row):
    return jnp.where(row >= step, pltpu.roll(array, step, 0), 0.0)


def taps_sum(array, taps):
    taps = taps.astype(F32)
    width = taps.shape[0]
    row = lax.broadcasted_iota(jnp.int32, array.shape, 0)
    total = jnp.zeros_like(array)
    for offset in range(width):
        back = width - 1 - offset
        moved = array if back == 0 else shifted(array, back, row)
        total = total + moved * taps[offset : offset + 1]
    return total


def whole_layer(
    sizes,
    features,
    first_gain,
    weights,
    shift,
    spike,
    scale,
    second_gain,
    content_taps,
    switch_taps,
):
    n_rep, n_fs, n_tp = sizes
    outer, inner = factor(n_fs)
    n_pair = pair_size(outer)
    members = n_rep * n_pair
    length, columns = features.shape
    wide = columns * n_tp
    rows = length * inner
    tokens = length * members
    key_lanes = weights[0].shape[1] // inner
    heads = key_lanes // HEAD_K
    value_lanes = heads * HEAD_V
    units = weights[6].shape[1] // members
    side = weights[5].shape[1]
    runs = outer // n_tp
    aligned = runs == n_pair
    pieces = pieces_of(length, 4)

    firsts = (0, 1, 3, 2, 4, 5)
    widths = [weights[w].shape[1] // inner for w in range(5)]
    offsets = [sum(widths[:w]) for w in range(5)]
    shard = weights[0].shape[0]
    result_rows = weights[5].shape[0] // inner
    down_rows = weights[8].shape[0] // members
    split = pieces_of(shard, 2)
    chunks = [(w, k * (shard // split), shard // split) for k in range(split) for w in (6, 7)]
    split = pieces_of(down_rows, members)
    size = down_rows // split
    chunks += [(8, k * size, size) for k in range(split)]
    count = len(chunks)

    def kernel(*refs):
        sources = refs[:9]
        (features_ref, gain_ref, shift_ref, spike_ref, scale_ref) = refs[9:14]
        (second_ref, content_taps_ref, switch_taps_ref, out_ref) = refs[14:18]
        (project_all, result_all, expand_all, contract_all) = refs[18:22]
        (whole_ref, normed_ref, spike_all, gated_ref, stage, slot_a, held, slot_b) = refs[22:30]
        (mid_all, normed_mid, hidden_ref, down_stage, slot_d, own_part, held_down, slot_c) = refs[
            30:38
        ]
        (far_send, far_recv, near_send, near_recv, own_sem) = refs[38:43]
        (spike_send, spike_recv, mix_send, mix_recv, cross_send, cross_recv) = refs[43:49]
        (group_send, group_recv, y_send, y_recv, z_send, z_recv) = refs[49:55]
        second_spread = refs[55:61]
        (down_send, down_recv, back_send, back_recv, pass_send, held_twin) = refs[61:67]
        (x_send, x_recv, first_sem, gain_rows) = refs[67:71]
        rep, fs, tp = lax.axis_index("rep"), lax.axis_index("fs"), lax.axis_index("tp")
        a, b = fs // inner, lax.rem(fs, inner)
        p = lax.rem(a, n_pair)
        far = [partner(a, d, outer) for d in range(1, outer)]
        near = [a * inner + lax.rem(b + d, inner) for d in range(1, inner)]
        tps = [lax.rem(tp + d, n_tp) for d in range(1, n_tp)]
        reps = [lax.rem(rep + d, n_rep) for d in range(1, n_rep)]
        sides = [lax.rem(b + d, inner) for d in range(1, inner)]
        group = [
            {"fs": a * inner + lax.rem(b + i, inner), "tp": lax.rem(tp + j, n_tp)}
            for i in range(inner)
            for j in range(n_tp)
            if i or j
        ]
        team = []
        diagonal = []
        for i in range(n_rep):
            for j in range(n_pair):
                if i or j:
                    r, q = lax.rem(rep + i, n_rep), lax.rem(p + j, n_pair)
                    peer = {"rep": r, "fs": (a - p + q) * inner + b}
                    team.append((peer, r * n_pair + q))
                    if i and j:
                        diagonal.append(peer)
        me = rep * n_pair + p
        twin = rep * n_pair + lax.rem(p + 1, n_pair)
        twin_peer = {"fs": (a - p + lax.rem(p + 1, n_pair)) * inner + b}
        between = lax.rem(a + 1, outer) // 2 == 1
        greeted = [{"fs": index * inner + b} for index in far]
        greeted += group + diagonal + [{"rep": index} for index in reps]
        barrier = pltpu.get_barrier_semaphore()
        for peer in greeted:
            pl.semaphore_signal(barrier, inc=1, device_id=peer, device_id_type=MESH)
        pl.semaphore_wait(barrier, len(greeted))

        def at(start, size):
            return pl.ds(pl.multiple_of(start, size), size)

        def source(c, position):
            w, start, size = chunks[c]
            member = rep * n_pair + lax.rem(position, n_pair)
            if w < 8:
                return sources[w].at[pl.ds(start, size), at(member * units, units)]
            base = pl.multiple_of(member * down_rows, down_rows)
            return sources[w].at[pl.ds(base + start, size), :]

        def block(c, index):
            w, start, size = chunks[c]
            if w < 8:
                base = pl.multiple_of(index * shard, shard)
                return expand_all.at[pl.ds(base + start, size), pl.ds((w - 6) * units, units)]
            return contract_all.at[pl.ds(start, size), at(index * side, side)]

        def origin(k, lanes_of, planes=n_rep):
            w = firsts[k]
            size = (result_rows if w == 5 else shard) // planes
            start = rep * size if planes > 1 else 0
            if w == 5:
                return sources[w].at[at(lanes_of * result_rows + start, size), :]
            return sources[w].at[at(start, size), at(lanes_of * widths[w], widths[w])]

        def landing(k, index, planes=n_rep):
            w = firsts[k]
            size = (result_rows if w == 5 else shard) // planes
            start = rep * size if planes > 1 else 0
            if w == 5:
                return result_all.at[at(start, size), at(index * side, side)]
            return project_all.at[at(index * shard + start, size), pl.ds(offsets[w], widths[w])]

        sent, passed = [], []
        near_copies, own_copies = {}, {}

        def send_far(c, d, slot, position):
            copy = send_to(
                source(c, position),
                block(c, fs),
                far_send.at[c, d],
                far_recv.at[c, slot],
                {"fs": position * inner + b},
            )
            sent.append(copy)

        def launch_far(c, steps):
            for d in steps:
                send_far(c, d, d, far[d])

        def beside(c):
            return pltpu.make_async_remote_copy(
                src_ref=source(c, far[0]),
                dst_ref=block(c, fs),
                send_sem=far_send.at[c, 0],
                recv_sem=far_recv.at[c, 0],
                device_id={"fs": far[0] * inner + b},
                device_id_type=MESH,
            )

        def launch_early(c):
            if not relayed:
                launch_far(c, every)
                return
            send_far(c, 1, jnp.where(between, 2, 1), jnp.where(between, far[2], far[1]))
            sent.append(beside(c))

            @pl.when(jnp.logical_not(between))
            def _():
                beside(c).start()

        def launch_late(c):
            if not relayed:
                return
            send_far(c, 2, jnp.where(between, 1, 2), jnp.where(between, far[1], far[2]))

            @pl.when(between)
            def _():
                beside(c).start()

        def landed_far(c, d):
            landed = block(c, far[d] * inner + b)
            pltpu.make_async_remote_copy(
                src_ref=landed,
                dst_ref=landed,
                send_sem=far_send.at[c, d],
                recv_sem=far_recv.at[c, d],
                device_id={"fs": far[d] * inner + b},
                device_id_type=MESH,
            ).wait_recv()
            return landed

        def launch_near(c):
            near_copies[c] = [
                send_to(
                    source(c, a),
                    block(c, fs),
                    near_send.at[c, 0, e],
                    near_recv.at[c, 0, e],
                    {"fs": index},
                )
                for e, index in enumerate(near)
            ]
            for d, position in enumerate(far):
                landed = block(c, position * inner + b)
                near_copies[c] += [
                    pltpu.make_async_remote_copy(
                        src_ref=landed,
                        dst_ref=landed,
                        send_sem=near_send.at[c, d + 1, e],
                        recv_sem=near_recv.at[c, d + 1, e],
                        device_id={"fs": index},
                        device_id_type=MESH,
                    )
                    for e, index in enumerate(near)
                ]
            sent.extend(near_copies[c])
            own_copies[c] = pltpu.make_async_copy(source(c, a), block(c, fs), own_sem.at[c])
            own_copies[c].start()

        def forward(c):
            for d in range(outer - 1):
                landed_far(c, d)
                for e in range(inner - 1):
                    near_copies[c][(d + 1) * (inner - 1) + e].start()

        def arrived(c):
            for copy in near_copies[c]:
                copy.wait_recv()
            own_copies[c].wait()

        third = [c for c in range(count) if chunks[c][0] < 8]
        fourth = [c for c in range(count) if chunks[c][0] == 8]
        relayed = outer == 4
        every = range(outer - 1)

        parts = [(h * (length // pieces), length // pieces) for h in range(pieces)]

        def spread(ref, sems):
            pair_send, pair_recv, across_send, across_recv, strip_send, strip_recv = sems
            pair_copies, across_copies, strip_copies = {}, {}, []

            def rows_of(member, h):
                start, size = parts[h]
                base = pl.multiple_of(member * length, length)
                return ref.at[pl.ds(base + start, size), at(tp * columns, columns)]

            def across(j, h):
                member = rep * n_pair + lax.rem(p + n_pair - j, n_pair)
                for i, index in enumerate(reps):
                    copy = send_to(
                        rows_of(member, h),
                        rows_of(member, h),
                        across_send.at[i, j, h],
                        across_recv.at[i, j, h],
                        {"rep": index},
                    )
                    across_copies[i, j, h] = copy
                    sent.append(copy)

            def strips(member):
                strip = ref.at[at(member * length, length), at(tp * columns, columns)]
                k = len(strip_copies)
                copies = [
                    send_to(strip, strip, strip_send.at[k, d], strip_recv.at[k, d], {"tp": index})
                    for d, index in enumerate(tps)
                ]
                strip_copies.append((member, copies))
                sent.extend(copies)

            def begin():
                for h in range(pieces):
                    for j in range(1, n_pair):
                        index = (a - p + lax.rem(p + j, n_pair)) * inner + b
                        copy = send_to(
                            rows_of(me, h),
                            rows_of(me, h),
                            pair_send.at[j - 1, h],
                            pair_recv.at[j - 1, h],
                            {"fs": index},
                        )
                        pair_copies[j, h] = copy
                        sent.append(copy)
                for h in range(pieces):
                    across(0, h)
                strips(me)

            def relay(h):
                for j in range(1, n_pair):
                    pair_copies[j, h].wait_recv()
                    across(j, h)
                    if h == pieces - 1:
                        strips(rep * n_pair + lax.rem(p + n_pair - j, n_pair))

            def complete(j):
                for i in range(1, n_rep):
                    for h in range(pieces):
                        across_copies[i - 1, j, h].wait_recv()
                    r = lax.rem(rep + n_rep - i, n_rep)
                    strips(r * n_pair + lax.rem(p + n_pair - j, n_pair))

            return begin, relay, complete, strip_copies

        y_copies, x_copies, first_copies = {}, {}, []

        def shard_of(e, d):
            position = a if d == 0 else far[d - 1]
            return position * inner + lax.rem(b + inner - e, inner)

        def aside(k):
            for e, index in enumerate(sides):
                y_copies[k, e + 1] = send_to(
                    origin(k, index, 1),
                    landing(k, fs, 1),
                    y_send.at[k, e],
                    y_recv.at[k, e],
                    {"fs": a * inner + index},
                )
                sent.append(y_copies[k, e + 1])
            copy = pltpu.make_async_copy(
                origin(k, b, 1), landing(k, fs, 1), first_sem.at[k]
            )
            copy.start()
            first_copies.append(copy)

        def along(k, e):
            index = shard_of(e, 0)
            start = landing(k, index) if e else origin(k, b)
            if relayed:
                middle = (jnp.where(between, 2, 1), jnp.where(between, far[2], far[1]))
                steps = [(0, 0, far[0]), (1,) + middle]
            else:
                steps = [(d, d, far[d]) for d in every]
            for d, slot, position in steps:
                copy = send_to(
                    start,
                    landing(k, index),
                    z_send.at[k, e, d],
                    z_recv.at[k, e, slot],
                    {"fs": position * inner + b},
                )
                sent.append(copy)

        def line_copy(k, e, d, send_sem, slot):
            landed = landing(k, shard_of(e, d + 1))
            return pltpu.make_async_remote_copy(
                src_ref=landed,
                dst_ref=landed,
                send_sem=send_sem,
                recv_sem=z_recv.at[k, e, slot],
                device_id={"fs": far[0] * inner + b},
                device_id_type=MESH,
            )

        def passed_on(k, e, d):
            return line_copy(k, e, d, pass_send.at[k, e, d], 3 - d)

        def carry_on(k, t, sources_of):
            for e in sources_of:
                slot, position = t, far[t]
                if relayed:
                    slot = jnp.where(between, 2 - t, t)
                    position = jnp.where(between, far[2 - t], far[t])
                landed = landing(k, position * inner + lax.rem(b + inner - e, inner))
                pltpu.make_async_remote_copy(
                    src_ref=landed,
                    dst_ref=landed,
                    send_sem=z_send.at[k, e, 0],
                    recv_sem=z_recv.at[k, e, slot],
                    device_id={"fs": far[0] * inner + b},
                    device_id_type=MESH,
                ).wait_recv()
                if relayed and t < 2:
                    passed.append((k, e, 2 - t))

                    @pl.when(between)
                    def _():
                        passed_on(k, e, 2 - t).start()

                for i, index in enumerate(reps):
                    x_copies[k, e, t, i] = send_to(
                        landed,
                        landed,
                        x_send.at[k, e, t, i],
                        x_recv.at[k, e, t, i],
                        {"rep": index},
                    )
                    sent.append(x_copies[k, e, t, i])

        def settled(k):
            first_copies[k].wait()
            for (at_k, e, d, i), copy in x_copies.items():
                if at_k == k:
                    copy.wait_recv()

        for k in range(len(firsts)):
            aside(k)
            along(k, 0)
        spot = whole_ref.at[at(b * length, length), at(tp * columns, columns)]
        own_features = pltpu.make_async_copy(features_ref, spot, own_sem.at[count])
        own_features.start()
        group_copies = [
            send_to(
                features_ref,
                spot,
                group_send.at[e, 0],
                group_recv.at[e, 0],
                {"fs": a * inner + index},
            )
            for e, index in enumerate(sides)
        ]
        lines = spike_all.at[at(b * length, length), :]
        own_spike = pltpu.make_async_copy(
            spike_ref.at[:, at(b * key_lanes, key_lanes)], lines, own_sem.at[count + 1]
        )
        own_spike.start()
        spike_copies = [
            send_to(
                spike_ref.at[:, at(index * key_lanes, key_lanes)],
                lines,
                spike_send.at[d],
                spike_recv.at[d],
                {"fs": a * inner + index},
            )
            for d, index in enumerate(sides)
        ]
        for k in range(len(firsts)):
            for e in range(1, inner):
                y_copies[k, e].wait_recv()
                along(k, e)
            carry_on(k, 0, range(1))
        for c in third:
            launch_early(c)
        for c in third + fourth:
            launch_near(c)
        for k in range(len(firsts)):
            carry_on(k, 0, range(1, inner))
        own_features.wait()
        strip_copies = []
        for e in range(inner):
            if e:
                group_copies[e - 1].wait()
            strip = whole_ref.at[
                at(lax.rem(b + inner - e, inner) * length, length), at(tp * columns, columns)
            ]
            strip_copies += [
                send_to(
                    strip, strip, group_send.at[e, d + 1], group_recv.at[e, d + 1], {"tp": index}
                )
                for d, index in enumerate(tps)
            ]
        for k in range(len(firsts)):
            for t in every[1:]:
                carry_on(k, t, range(inner))
        gain_rows[...] = jnp.broadcast_to(
            scale_ref[...].astype(F32).reshape(1, -1), gain_rows.shape
        )
        own_spike.wait()
        for copy in strip_copies + spike_copies:
            copy.wait()

        def first_norm(i, carry):
            lines = at(i * length, length)
            normed_ref[lines, :] = row_norm(whole_ref[lines, :], gain_ref[...].reshape(1, -1))
            return carry

        lax.fori_loop(0, inner, first_norm, 0)
        for c in third:
            launch_late(c)
        for c in fourth:
            launch_early(c)
        def forwards(middle, ends):
            if not relayed:
                for c in ends:
                    forward(c)
                return

            def each(chosen):
                def send():
                    for c in chosen:
                        forward(c)

                return send

            if middle:
                pl.when(between)(each(middle))
            if ends:
                pl.when(jnp.logical_not(between))(each(ends))

        half = len(third) // 2
        forwards(third[:half], [])
        for k in range(len(firsts)):
            if firsts[k] != 5:
                settled(k)

        def attention(index):
            lines = at(index * length, length)
            sums = jnp.dot(normed_ref[lines, :], project_all[...], preferred_element_type=F32)
            gated_ref[lines, :] = attend_rows(
                sums,
                shift_ref[:, at(b * key_lanes, key_lanes)],
                spike_all[lines, :],
                gain_rows[:1, at(b * value_lanes, value_lanes)],
                heads,
            )

        order = sides + [b]
        for index in order[:1]:
            attention(index)
        settled(firsts.index(5))

        def mixed(index, strip):
            return jnp.dot(
                gated_ref[at(index * length, length), :],
                result_all[:, at(strip * columns, columns)],
                preferred_element_type=F32,
            )

        mix_copies, cross_copies = [], []

        def mix_strips(i):
            copies = []
            for d, other in enumerate(tps):
                stage[i, d] = mixed(order[i], other).astype(BF16)
                copies.append(
                    send_to(
                        stage.at[i, d],
                        slot_a.at[i, d],
                        mix_send.at[i, d],
                        mix_recv.at[i, d],
                        {"tp": other},
                    )
                )
            mix_copies.append(copies)
            sent.extend(copies)

        def mix_sum(i):
            total = mixed(order[i], tp)
            for d, copy in enumerate(mix_copies[i]):
                copy.wait_recv()
                total = total + slot_a[i, d].astype(F32)
            return total

        for i in range(inner):
            if i:
                attention(order[i])
            mix_strips(i)
            if i < inner - 1:
                held[i] = mix_sum(i).astype(BF16)
                copy = send_to(
                    held.at[i],
                    slot_b.at[i],
                    cross_send.at[i],
                    cross_recv.at[i],
                    {"fs": a * inner + order[i]},
                )
                cross_copies.append(copy)
                sent.append(copy)

        forwards(third[half:], third[:1])
        total = mix_sum(inner - 1)
        for d, copy in enumerate(cross_copies):
            copy.wait_recv()
            total = total + slot_b[d].astype(F32)
        base = whole_ref[at(b * length, length), at(tp * columns, columns)].astype(F32)
        mine = mid_all.at[at(me * length, length), at(tp * columns, columns)]
        mine[...] = (base + total.astype(BF16).astype(F32)).astype(BF16)

        begin, relay, complete, blocks = spread(mid_all, second_spread)
        begin()
        forwards([], third[1:])
        for h in range(pieces):
            relay(h)
        for c in fourth:
            launch_late(c)
        forwards(fourth, fourth[:1])
        for j in range(n_pair):
            complete(j)

        def second_norm(member):
            lines = at(member * length, length)
            normed_mid[lines, :] = row_norm(mid_all[lines, :], second_ref[...].reshape(1, -1))

        forwards([], fourth[1:2])
        for member, copies in blocks:
            for copy in copies:
                copy.wait_recv()
            second_norm(member)
        forwards([], fourth[2:3])
        for c in third:
            arrived(c)

        def expand(i, carry):
            lines = at(i * length, length)
            both = jnp.dot(normed_mid[lines, :], expand_all[...], preferred_element_type=F32)
            both = both.astype(BF16).astype(F32)
            value = taps_sum(both[:, :units], content_taps_ref[:, at(me * units, units)])
            gate = taps_sum(both[:, units:], switch_taps_ref[:, at(me * units, units)])
            hidden_ref[lines, :] = (value * jax.nn.gelu(gate, approximate=True)).astype(BF16)
            return carry

        lax.fori_loop(0, 1, expand, 0)
        forwards([], fourth[3:])
        lax.fori_loop(1, members, expand, 0)

        back_copies = {}
        pending, turning = [], []

        def finish(e, run, place, lanes, copies):
            total = own_part[:, lanes]
            for d, copy in enumerate(copies):
                copy.wait_recv()
                total = total + slot_d[d, :, lanes].astype(F32)
            own_part[:, lanes] = total
            held_down[:, lanes] = total.astype(BF16)
            for k, (i, j, member) in enumerate(phases(e, run)[0]):
                back_copies[e, run, k] = send_to(
                    held_down.at[at(member * length, length), lanes],
                    slot_c.at[k, :, lanes],
                    back_send.at[e, place, k],
                    back_recv.at[e, place, k],
                    peer_of(i, j),
                )

        def peer_of(i, j):
            return {"rep": reps[i - 1]} if i else twin_peer

        def phases(e, run):
            def member(i, j):
                return lax.rem(rep + i, n_rep) * n_pair + lax.rem(p + j, n_pair)

            hops = [(i, 0, member(i, j)) for j in (1, 0) for i in range(1, n_rep)]
            return hops, [(0, 1, member(0, 1))]

        def turned(e, run, place, lanes):
            hops, turns = phases(e, run)
            for n, (i, j, member) in enumerate(turns):
                total = own_part[at(member * length, length), lanes]
                for k in range(n_rep - 1):
                    back_copies[e, run, k].wait_recv()
                    total = total + slot_c[k, :, lanes].astype(F32)
                held_twin[n, :, lanes] = total.astype(BF16)
                back_copies[e, run, len(hops) + n] = send_to(
                    held_twin.at[n, :, lanes],
                    slot_c.at[len(hops) + n, :, lanes],
                    back_send.at[e, place, len(hops) + n],
                    back_recv.at[e, place, len(hops) + n],
                    peer_of(i, j),
                )

        for e in range(inner):
            lane = lax.rem(b + inner - e, inner)
            waited = set()

            def weights_of(run):
                for c in fourth:
                    for d in range(run, outer, runs) if aligned else range(outer):
                        if (c, d) in waited:
                            continue
                        waited.add((c, d))
                        if e:
                            near_copies[c][d * (inner - 1) + e - 1].wait_recv()
                        elif d == 0:
                            own_copies[c].wait()

            def spot(run):
                place = lax.rem(p + run, runs) if aligned else run
                return place, at((place * inner + lane) * side, side)

            def product(strip, place):
                index = (strip * runs + place) * inner + lane
                return jnp.dot(
                    hidden_ref[...],
                    contract_all[:, at(index * side, side)],
                    preferred_element_type=F32,
                )

            for run in range(runs):
                weights_of(run)
                place, lanes = spot(run)
                copies = []
                for d, other in enumerate(tps):
                    down_stage[d, :, lanes] = product(other, place).astype(BF16)
                    copies.append(
                        send_to(
                            down_stage.at[d, :, lanes],
                            slot_d.at[d, :, lanes],
                            down_send.at[e, run, d],
                            down_recv.at[e, run, d],
                            {"tp": other},
                        )
                    )
                sent.extend(copies)
                own_part[:, lanes] = product(tp, place)
                for step in turning:
                    turned(*step[:4])
                turning = pending
                for step in pending:
                    finish(*step)
                pending = [(e, run, place, lanes, copies)]
        for step in pending:
            finish(*step)
        for step in turning + pending:
            turned(*step[:4])
        for e in range(inner):
            for run in range(runs):
                lane = lax.rem(b + inner - e, inner)
                lanes = at((lax.rem(p + run, runs) if aligned else run) * inner * side + lane * side, side)
                total = own_part[at(me * length, length), lanes]
                for k in range(n_rep - 1, members - 1):
                    back_copies[e, run, k].wait_recv()
                    total = total + slot_c[k, :, lanes].astype(F32)
                base = mine[:, lanes].astype(F32)
                out_ref[:, lanes] = (base + total.astype(BF16).astype(F32)).astype(BF16)
        for copy in sent + list(back_copies.values()):
            copy.wait_send()
        if passed:

            @pl.when(between)
            def _():
                for step in passed:
                    passed_on(*step).wait_send()

    dma = pltpu.SemaphoreType.DMA
    vmem = pl.BlockSpec(memory_space=pltpu.VMEM)
    hbm = pl.BlockSpec(memory_space=pl.ANY)

    def pair(*shape):
        shape = tuple(max(n, 1) for n in shape)
        return [dma(shape), dma(shape)]

    def room(*shape, dtype=BF16):
        return pltpu.VMEM(tuple(max(n, 1) for n in shape), dtype)

    scratch = [
        room(shard * n_fs, sum(widths)),
        room(result_rows, side * n_fs),
        room(shard * n_fs, 2 * units),
        room(down_rows, side * n_fs),
        room(rows, wide),
        room(rows, wide),
        room(rows, key_lanes, dtype=F32),
        room(rows, value_lanes),
        room(inner, n_tp - 1, length, columns),
        room(inner, n_tp - 1, length, columns),
        room(inner - 1, length, columns),
        room(inner - 1, length, columns),
        room(tokens, wide),
        room(tokens, wide),
        room(tokens, units),
        room(n_tp - 1, tokens, columns),
        room(n_tp - 1, tokens, columns),
        room(tokens, columns, dtype=F32),
        room(tokens, columns),
        room(members - 1, length, columns),
    ]
    scratch += pair(count, outer - 1) + pair(count, outer, inner - 1) + [dma((count + 2,))]
    many = len(firsts)
    scratch += pair(inner - 1) + pair(inner, n_tp - 1) + pair(inner - 1)
    scratch += pair(inner, n_tp) + pair(many, inner - 1) + pair(many, inner, outer - 1)
    scratch += pair(n_pair - 1, pieces) + pair(n_rep - 1, n_pair, pieces)
    scratch += pair(members, n_tp - 1)
    scratch += pair(inner, runs, n_tp - 1) + pair(inner, runs, members - 1)
    scratch += [dma((many, inner, max(outer - 1, 1))), room(n_rep - 1, length, columns)]
    scratch += pair(many, inner, outer - 1, n_rep - 1) + [dma((many,))]
    scratch.append(room(8, scale.shape[0], dtype=F32))
    return pl.pallas_call(
        kernel,
        out_shape=jax.ShapeDtypeStruct((length, columns), BF16),
        in_specs=[hbm] * 10 + [vmem] * 7,
        out_specs=vmem,
        scratch_shapes=scratch,
        compiler_params=pltpu.CompilerParams(
            collective_id=0, has_side_effects=True, vmem_limit_bytes=VMEM_LIMIT
        ),
        name="whole_layer",
    )(
        *weights,
        features,
        first_gain,
        shift.reshape(1, -1),
        spike,
        scale,
        second_gain,
        content_taps,
        switch_taps,
    )


def shards(
    sizes,
    incoming_features,
    attend_prenormal_scale,
    probe_matrix,
    lookup_matrix,
    content_matrix,
    forgetting_matrix,
    result_switch_matrix,
    forgetting_shift,
    spike_forget_logarithm,
    attend_unit_scale,
    attend_result_matrix,
    perceptron_scale,
    content_expand_matrix,
    switch_expand_matrix,
    content_kernel,
    switch_kernel,
    contract_matrix,
):
    n_rep, n_fs, n_tp = sizes
    rep = lax.axis_index("rep")
    length = incoming_features.shape[0]
    if fits(
        sizes, incoming_features, probe_matrix, attend_result_matrix, content_expand_matrix
    ):
        return whole_layer(
            sizes,
            incoming_features,
            attend_prenormal_scale,
            (
                probe_matrix,
                lookup_matrix,
                content_matrix,
                forgetting_matrix,
                result_switch_matrix,
                attend_result_matrix,
                content_expand_matrix,
                switch_expand_matrix,
                contract_matrix,
            ),
            forgetting_shift,
            spike_forget_logarithm,
            attend_unit_scale,
            perceptron_scale,
            content_kernel,
            switch_kernel,
        )

    def mine(array, axis):
        size = array.shape[axis] // n_rep
        return lax.dynamic_slice_in_dim(array, rep * size, size, axis)

    project = jnp.concatenate(
        [
            mine(matrix, 1)
            for matrix in (
                probe_matrix,
                lookup_matrix,
                content_matrix,
                forgetting_matrix,
                result_switch_matrix,
            )
        ],
        axis=1,
    )
    spike_all = lax.all_to_all(
        spike_forget_logarithm, "rep", split_axis=1, concat_axis=0, tiled=True
    )
    expand = jnp.concatenate([mine(content_expand_matrix, 1), mine(switch_expand_matrix, 1)], axis=1)
    side = attend_result_matrix.shape[1]
    inside = side % 128 == 0
    outs = first_half(
        project,
        mine(attend_result_matrix, 0),
        expand,
        mine(contract_matrix, 0),
        incoming_features,
        attend_prenormal_scale,
        mine(forgetting_shift, 0),
        spike_all,
        mine(attend_unit_scale, 0),
        1 if inside else 0,
        inside,
        sizes,
    )
    if inside:
        expand_all, contract_all, middle, whole_mid = outs
    else:
        expand_all, contract_all, result_all, switched_result = outs
        result_all, contract_all = (
            array.reshape(n_fs, -1, side).swapaxes(0, 1).reshape(-1, n_fs * side)
            for array in (result_all, contract_all)
        )
        mixer_partial = jnp.dot(switched_result, result_all, preferred_element_type=F32)
        middle, whole_mid = reduce_group(
            mixer_partial.astype(BF16), incoming_features, sizes, True, 2
        )
    normed_mid = row_norm(whole_mid, perceptron_scale)
    both = jnp.dot(normed_mid, expand_all, preferred_element_type=F32).astype(BF16)
    half = both.shape[1] // 2
    conv_value = causal_conv(both[:, :half], mine(content_kernel, 1), length)
    conv_gated = causal_conv(both[:, half:], mine(switch_kernel, 1), length)
    hidden = (conv_value * jax.nn.gelu(conv_gated, approximate=True)).astype(BF16)
    down_partial = jnp.dot(hidden, contract_all, preferred_element_type=F32).astype(BF16)
    return reduce_group(down_partial, middle, sizes, False, 3)[0]


def solution(mesh):
    sizes = (mesh.shape["rep"], mesh.shape["fs"], mesh.shape["tp"])
    placed = (
        P(("rep", "fs"), "tp"),
        P(),
        P("fs", "tp"),
        P("fs", "tp"),
        P("fs", "tp"),
        P("fs", "tp"),
        P("fs", "tp"),
        P("tp"),
        P(("rep", "fs"), "tp"),
        P("tp"),
        P("tp", "fs"),
        P(),
        P("fs", "tp"),
        P("fs", "tp"),
        P(None, "tp"),
        P(None, "tp"),
        P("tp", "fs"),
    )
    return jax.shard_map(
        functools.partial(shards, sizes),
        mesh=mesh,
        in_specs=placed,
        out_specs=P(("rep", "fs"), "tp"),
        check_vma=False,
    )
```
